128 devices in a mesh: sp: 16 (over z, x), fs: 4 (over y), tp: 2 (over core).
Axes of the slice: x: 4, y: 4, z: 4, core: 2. Of those that a mesh axis runs over, the one named last changes fastest.
Arguments:
- stream: bfloat16 [4, 16384, 2048], P('fs', 'sp', 'tp'), parts along dimension 0, may hold values from -6 to 6
- w_pool_in: bfloat16 [2048, 1024], P(None, 'tp'), may hold values from -0.125 to 0.125
- w_query: bfloat16 [2048, 1024], P(None, 'tp'), may hold values from -0.125 to 0.125
- w_forget: bfloat16 [2048, 1024], P(None, 'tp'), may hold values from -0.125 to 0.125
- w_value: bfloat16 [2048, 1024], P(None, 'tp'), may hold values from -0.125 to 0.125
- w_outgate: bfloat16 [2048, 1024], P(None, 'tp'), may hold values from -0.125 to 0.125
- pool_mix: bfloat16 [4, 256, 256], P('tp'), may hold values from -0.375 to 0.375
- pool_scale: float32 [1024], P('tp'), may hold values from 0.1 to 1.9
- lower_bound: float32 [1024], P('tp'), may hold values from 0.9 to 1
- extra_decay: float32 [16384, 8], P('sp', 'tp'), may hold values from -0.7 to 0
- rec_gain: float32 [128], replicated, may hold values from 0.1 to 1.9
- w_out_pool: bfloat16 [1024, 2048], P('tp'), may hold values from -0.125 to 0.125
- w_out_rec: bfloat16 [1024, 2048], P('tp'), may hold values from -0.125 to 0.125
- norm_gain: float32 [2048], P('tp'), may hold values from 0.1 to 1.9
- norm_bias: float32 [2048], P('tp'), may hold values from -3 to 3
Outputs:
- layer_out: bfloat16 [4, 16384, 2048], P('fs', 'sp', 'tp'), parts along dimension 0
The draws below stay inside these ranges and needn't reach their ends.
There are 4 independent parts, one for each index of `fs`. The reference program is written for one: setup_inputs(seed, part) draws one part's arguments, and reference() takes and returns one part's arrays. A program takes and returns all parts, laid end to end along the dimension named above; an argument that names none is the same for every part. Nothing has to cross between parts.
All inputs are finite; a program needn't handle non-finite values.
Results may differ from the reference program's by a relative error of at most 0.0085.
Values may be sent and summed in bfloat16 or wider, within the bound.
No kernel may reach another device: no remote copies, remote signals or barrier semaphores. Data moves between devices by JAX's collectives and lax.ppermute only.
A program may use at most 128 MiB of HBM per device.

```python
import math
import jax
import jax.numpy as jnp
from jax import lax

D = 2048
POOL_W = 1024
REC_W = 1024
DK = 128
WMAX = 16
BLOCK_ROWS = 128
TOK_DEV = 1024
GROUP_CH = 256
HEADS = 8
SEQ = 16384


def draw_lower_bound(key, part):
    key_order = jax.random.fold_in(key, 11)
    key_fast = jax.random.fold_in(key, 12)
    key_slow = jax.random.fold_in(key, 13)
    order = jax.random.permutation(key_order, HEADS)
    chosen = order < HEADS // 2
    fast_gap = jnp.exp(jax.random.uniform(key_fast, (HEADS, DK), jnp.float32, math.log(0.03), math.log(0.06)))
    slow_gap = jnp.exp(jax.random.uniform(key_slow, (HEADS, DK), jnp.float32, math.log(0.16 / SEQ), math.log(0.8 / SEQ)))
    gaps = jnp.where(chosen[:, None], fast_gap, slow_gap)
    return (1.0 - gaps).reshape(REC_W).astype(jnp.float32)


def draw_extra_decay(key, part):
    key_base = jax.random.fold_in(key, 21)
    key_where = jax.random.fold_in(key, 22)
    key_drop = jax.random.fold_in(key, 23)
    blocks = SEQ // TOK_DEV
    base = jnp.exp(jax.random.uniform(key_base, (blocks,), jnp.float32, math.log(0.04 / SEQ), math.log(0.2 / SEQ)))
    base_rows = jnp.repeat(base, TOK_DEV)
    places = jax.random.randint(key_where, (2,), 0, SEQ)
    marked = jnp.any(jnp.arange(SEQ)[:, None] == places[None, :], axis=1)
    drops = jax.random.uniform(key_drop, (SEQ, HEADS), jnp.float32, 0.22, 0.69)
    total = base_rows[:, None] + jnp.where(marked[:, None], drops, jnp.float32(0.0))
    return (-total).astype(jnp.float32)


def shard_levels(rng, shape, split, least, largest):
    gain = 1.0
    for axis_at, parts in split:
        draws = jax.random.uniform(jax.random.fold_in(jax.random.fold_in(rng, 6), axis_at), (parts,), jnp.float32, least / len(split), largest / len(split))
        gain = gain * jnp.repeat(jnp.exp(draws), shape[axis_at] // parts).reshape((-1,) + (1,) * (len(shape) - 1 - axis_at))
    return gain


def normal_values(key, dims, width, bound, shards=(), dtype=jnp.bfloat16):
    factor_of = shard_levels(key, dims, shards, -0.22, 0.18) if shards else 1.0
    result = jax.random.normal(key, dims, jnp.float32) * width * factor_of
    return jnp.minimum(jnp.maximum(result, -bound), bound).astype(dtype)


def setup_inputs(seed: int = 0, part: int = 0) -> dict:
    key_list = jax.random.split(jax.random.key(seed), 16)
    own_keys = jax.random.split(jax.random.fold_in(key_list[15], part), 16)
    return {
        "stream": normal_values(own_keys[0], (1, SEQ, D), 1.0, 6.0, ((1, 16), (2, 2))),
        "w_pool_in": normal_values(key_list[1], (D, POOL_W), D ** -0.5, 0.125, ((1, 2),)),
        "w_query": normal_values(key_list[2], (D, REC_W), D ** -0.5, 0.125, ((1, 2),)),
        "w_forget": normal_values(key_list[3], (D, REC_W), D ** -0.5, 0.125, ((1, 2),)),
        "w_value": normal_values(key_list[4], (D, REC_W), D ** -0.5, 0.125, ((1, 2),)),
        "w_outgate": normal_values(key_list[5], (D, REC_W), D ** -0.5, 0.125, ((1, 2),)),
        "pool_mix": normal_values(key_list[6], (4, GROUP_CH, GROUP_CH), GROUP_CH ** -0.5, 0.375, ((0, 2),)),
        "pool_scale": jnp.clip(1.0 + 0.18 * jax.random.normal(key_list[7], (POOL_W,), jnp.float32), 0.1, 1.9),
        "lower_bound": draw_lower_bound(jax.random.fold_in(key_list[15], 71), part),
        "extra_decay": draw_extra_decay(jax.random.fold_in(key_list[15], 71), part),
        "rec_gain": jnp.clip(1.0 + 0.18 * jax.random.normal(key_list[10], (DK,), jnp.float32), 0.1, 1.9),
        "w_out_pool": normal_values(key_list[11], (POOL_W, D), (POOL_W + REC_W) ** -0.5, 0.125, ((0, 2),)),
        "w_out_rec": normal_values(key_list[12], (REC_W, D), (POOL_W + REC_W) ** -0.5, 0.125, ((0, 2),)),
        "norm_gain": jnp.clip(1.0 + 0.18 * jax.random.normal(key_list[13], (D,), jnp.float32), 0.1, 1.9),
        "norm_bias": normal_values(key_list[14], (D,), 0.5, 3.0, ((0, 2),), jnp.float32),
    }


ALPHA = 2.0 ** 0.25
EPS_RMS = 1e-06
EPS_NORM = 1e-05
HIGHEST = lax.Precision.HIGHEST

def pool_branch(pooled, pool_mix, pool_scale):
    length = pooled.shape[0]
    data = pooled.astype(jnp.float32)
    padded = jnp.pad(data, ((WMAX - 1, 0), (0, 0)))
    group_id = jnp.arange(POOL_W).astype(jnp.int32) // GROUP_CH
    window_len = jnp.left_shift(jnp.ones_like(group_id), group_id + 1)
    window_sum = jnp.zeros((length, POOL_W), jnp.float32)
    for lag_rows in range(WMAX):
        lagged = padded[WMAX - 1 - lag_rows:WMAX - 1 - lag_rows + length]
        window_sum = window_sum + jnp.where(lag_rows < window_len[None, :], lagged, jnp.float32(0.0))
    position = jnp.arange(1, length + 1).astype(jnp.float32)
    counts = jnp.minimum(position[:, None], window_len.astype(jnp.float32)[None, :])
    pool_diff = (window_sum / counts - data).astype(jnp.bfloat16)
    grouped = pool_diff.reshape(length, 4, GROUP_CH).astype(jnp.float32)
    mixed = jnp.einsum('tgc,gcd->tgd', grouped, pool_mix.astype(jnp.float32))
    return (mixed.reshape(length, POOL_W) * pool_scale).astype(jnp.bfloat16)

def recurrent_branch(queries, forget_in, value_in, gate_in, lower_bound, extra_decay, rec_gain):
    length = queries.shape[0]
    blocks = length // BLOCK_ROWS
    forget = lower_bound + (1.0 - lower_bound) * jax.nn.sigmoid(forget_in.astype(jnp.float32))
    log_keep = jnp.log(forget).reshape(length, HEADS, DK) + extra_decay[:, :, None]
    weight_in = (1.0 - forget).reshape(length, HEADS, DK)
    gated_query = jax.nn.silu(queries.astype(jnp.float32)).reshape(length, HEADS, DK)
    values = value_in.reshape(length, HEADS, DK)

    def to_blocks(arr):
        return arr.reshape(blocks, BLOCK_ROWS, HEADS, DK)
    lower_mask = jnp.tril(jnp.ones((BLOCK_ROWS, BLOCK_ROWS), jnp.float32))

    def block_step(state, inputs):
        query_blk, keep_blk, input_blk, value_blk = inputs
        value_wide = value_blk.astype(jnp.float32)
        log_total = jnp.cumsum(keep_blk, axis=0)
        query_up = query_blk * jnp.exp(log_total)
        input_down = input_blk * jnp.exp(-log_total)
        scores = jnp.einsum('thd,shd->hts', query_up, input_down, precision=HIGHEST) * lower_mask[None]
        scores = scores.astype(jnp.bfloat16).astype(jnp.float32)
        inside = jnp.einsum('hts,she->the', scores, value_wide, precision=HIGHEST)
        carried = jnp.einsum('thd,hde->the', query_up, state, precision=HIGHEST)
        log_end = log_total[-1]
        in_weight = (input_blk * jnp.exp(log_end[None] - log_total)).astype(jnp.bfloat16).astype(jnp.float32)
        new_state = jnp.exp(log_end)[:, :, None] * state + jnp.einsum('shd,she->hde', in_weight, value_wide, precision=HIGHEST)
        return (new_state, inside + carried)
    start_state = jnp.zeros((HEADS, DK, DK), jnp.float32)
    _, outputs = lax.scan(block_step, start_state, (to_blocks(gated_query), to_blocks(log_keep), to_blocks(weight_in), to_blocks(values)))
    rec_raw = outputs.reshape(length, HEADS, DK)
    rec_norm = rec_raw * lax.rsqrt(lax.optimization_barrier(jnp.mean(rec_raw * rec_raw, axis=-1, keepdims=True)) + EPS_RMS) * rec_gain
    gated = rec_norm * jax.nn.silu(gate_in.astype(jnp.float32)).reshape(length, HEADS, DK)
    return gated.reshape(length, REC_W).astype(jnp.bfloat16)

def reference(stream, w_pool_in, w_query, w_forget, w_value, w_outgate, pool_mix, pool_scale, lower_bound, extra_decay, rec_gain, w_out_pool, w_out_rec, norm_gain, norm_bias):
    features = stream[0]

    def project(weight):
        return jnp.dot(features, weight, preferred_element_type=jnp.float32).astype(jnp.bfloat16)
    pooled = project(w_pool_in)
    queries = project(w_query)
    forget_in = project(w_forget)
    value_in = project(w_value)
    gate_in = project(w_outgate)
    pool_out = pool_branch(pooled, pool_mix, pool_scale)
    rec_out = recurrent_branch(queries, forget_in, value_in, gate_in, lower_bound, extra_decay, rec_gain)
    mix = jnp.dot(pool_out, w_out_pool, preferred_element_type=jnp.float32) + jnp.dot(rec_out, w_out_rec, preferred_element_type=jnp.float32)
    resid = ALPHA * features.astype(jnp.float32) + mix
    row_mean = lax.optimization_barrier(jnp.mean(resid, axis=-1, keepdims=True))
    row_var = lax.optimization_barrier(jnp.mean((resid - row_mean) * (resid - row_mean), axis=-1, keepdims=True))
    normed = (resid - row_mean) * lax.rsqrt(row_var + EPS_NORM) * norm_gain + norm_bias
    return normed.astype(jnp.bfloat16)[None]
```

```python
import functools

import jax
import jax.numpy as jnp
from jax import lax
from jax.experimental import pallas as pl
from jax.experimental.pallas import tpu as pltpu
from jax.sharding import Mesh
from jax.sharding import PartitionSpec as P

D = 2048
DK = 128
BLOCK = 128
MID = 63
HALO = 16
GROUP_CH = 256
SP = ("sp_0", "sp_1")
ALPHA = 2.0**0.25
EPS_RMS = 1e-06
EPS_NORM = 1e-05
F32 = jnp.float32
BF16 = jnp.bfloat16
MIB = 1 << 20

TP, ROW0, EARLY = 0, 1, 2


def mm(a, b):
    return jnp.dot(a, b, preferred_element_type=F32)


def mm_t(a, b, ca, cb):
    return lax.dot_general(a, b, (((ca,), (cb,)), ((), ())), preferred_element_type=F32)


def call(body, meta, args, in_specs, out_specs, out_shape, grid, scratch=(), vmem=20, flops=0, aliases=None):
    nbytes = sum(a.size * a.dtype.itemsize for a in args)
    return pl.pallas_call(
        body,
        grid_spec=pltpu.PrefetchScalarGridSpec(
            num_scalar_prefetch=1,
            grid=grid,
            in_specs=in_specs,
            out_specs=out_specs,
            scratch_shapes=list(scratch),
        ),
        out_shape=out_shape,
        input_output_aliases=aliases or {},
        compiler_params=pltpu.CompilerParams(
            dimension_semantics=("arbitrary",) * len(grid), vmem_limit_bytes=vmem * MIB
        ),
        cost_estimate=pl.CostEstimate(flops=flops, bytes_accessed=nbytes, transcendentals=0),
    )(meta, *args)


def rows_spec(rows, cols, first=0):
    return pl.BlockSpec((rows, cols), lambda i, m: (i + first, 0))


def whole(shape):
    return pl.BlockSpec(shape, lambda i, m: (0,) * len(shape))


def own_rows(rows, cols):
    return pl.BlockSpec((rows, cols), lambda i, m: (m[TP], 0))


def other_rows(rows, cols):
    return pl.BlockSpec((rows, cols), lambda i, m: (1 - m[TP], 0))


def own_cols(rows, cols):
    return pl.BlockSpec((rows, cols), lambda i, m: (0, m[TP]))


def partial_body(m, x, wf, wv, fo, vo):
    fo[...] = mm(x[...], wf[...])
    vo[...] = mm(x[...], wv[...])


def gates_body(
    heads, m, x, wf, wv, fp, vp, lb, ed, v_out, down_out, rel_out, st_out, c_out, pay_out, own_out, state, off
):
    i = pl.program_id(0)
    rows = x.shape[0]
    width = heads * DK

    @pl.when(i == 0)
    def _():
        state[...] = jnp.zeros_like(state)
        off[...] = jnp.zeros_like(off)

    f = (fp[...] + mm(x[...], wf[...])).astype(BF16).astype(F32)
    v = (vp[...] + mm(x[...], wv[...])).astype(BF16)
    v_out[...] = v
    low = lb[...]
    gap = 1.0 - low
    sig = jax.nn.sigmoid(f)
    weight = gap * (1.0 - sig)
    extra = ed[...]
    log_keep = jnp.log(low + gap * sig) + jnp.concatenate(
        [jnp.broadcast_to(extra[:, h : h + 1], (rows, DK)) for h in range(heads)], axis=1
    )
    hi = log_keep.astype(BF16)
    lo = (log_keep - hi.astype(F32)).astype(BF16)
    t_id = lax.broadcasted_iota(jnp.int32, (BLOCK, 2 * BLOCK), 0)
    s_id = lax.broadcasted_iota(jnp.int32, (BLOCK, 2 * BLOCK), 1)
    mask = (t_id >= jnp.where(s_id >= BLOCK, s_id - BLOCK, s_id)).astype(F32).astype(BF16)
    for b in range(rows // BLOCK):
        r = slice(b * BLOCK, (b + 1) * BLOCK)
        total = mm(mask, jnp.concatenate([hi[r], lo[r]], axis=0))
        middle = total[MID : MID + 1]
        end = total[BLOCK - 1 : BLOCK]
        rel = total - middle
        rel_out[r, :] = rel
        down = weight[r] * jnp.exp(-rel)
        down_out[r, :] = down.astype(BF16)
        in_weight = (down * jnp.exp(end - middle)).astype(BF16)
        e_mid, e_end = jnp.exp(middle), jnp.exp(end)
        before = off[...]
        c_out[pl.ds(i * (rows // BLOCK) + b, 1), :] = jnp.exp(middle + before)
        off[...] = before + end
        for h in range(heads):
            c = slice(h * DK, (h + 1) * DK)
            old = state[c, :]
            st_out[b * width + h * DK : b * width + (h + 1) * DK, :] = (old * e_mid[:, c]).astype(BF16)
            state[c, :] = old * e_end[:, c] + mm_t(v[r, c], in_weight[:, c], 0, 0)

    @pl.when(i == pl.num_programs(0) - 1)
    def _():
        write_payload(heads, state[...], jnp.exp(off[...]), pay_out, own_out)


def write_payload(heads, state, decay_row, pay_out, own_out):
    width = heads * DK
    decay = jnp.concatenate(
        [decay_row[:, h * DK : (h + 1) * DK] for h in range(heads)], axis=0
    )
    pack_payload(width, state, decay, pay_out)
    own_out[:width, :] = state
    own_out[width:, :] = jnp.concatenate([decay, jnp.zeros_like(decay)], axis=0)


def pack_payload(width, state, decay, pay_out):
    hi = decay.astype(BF16).astype(F32)
    pay_out[:width, :] = state.astype(BF16)
    pay_out[width:, :] = jnp.concatenate(
        [hi, decay - hi, jnp.zeros_like(hi), jnp.zeros_like(hi)], axis=0
    ).astype(BF16)


def unpack_decay(heads, width, ref):
    rows = ref[width:, :].astype(F32)
    return rows[:heads] + rows[heads : 2 * heads]


def combine_body(heads, which, m, own, pre, recv, pay_out, own_out, pre_out):
    width = heads * DK
    early = m[EARLY + which] == 1
    d_own = own[width : width + heads, :]
    d_pre = pre[width : width + heads, :]
    d_recv = unpack_decay(heads, width, recv)
    d_all = d_own * d_recv
    new_d_pre = jnp.where(early, d_recv * d_pre, d_pre)
    pre_out[width:, :] = jnp.concatenate([new_d_pre, jnp.zeros_like(d_pre)], axis=0)
    own_out[width:, :] = jnp.concatenate([d_all, jnp.zeros_like(d_all)], axis=0)
    states = []
    for h in range(heads):
        c = slice(h * DK, (h + 1) * DK)
        got = recv[c, :].astype(F32)
        mine = own[c, :]
        p = pre[c, :]
        pre_out[c, :] = jnp.where(early, p + d_pre[h : h + 1] * got, p)
        new = jnp.where(early, d_own[h : h + 1] * got + mine, d_recv[h : h + 1] * mine + got)
        own_out[c, :] = new
        states.append(new)
    pack_payload(width, jnp.concatenate(states, axis=0), d_all, pay_out)


def pool_body(m, xo, xp, to, tp, wo, wp, mix, scale, out, ext):
    i = pl.program_id(0)
    rows = xo.shape[0]

    @pl.when(i == 0)
    def _():
        ext[:HALO, :] = (mm(to[...], wo[...]) + mm(tp[...], wp[...])).astype(BF16)

    @pl.when(i > 0)
    def _():
        ext[:HALO, :] = ext[rows : rows + HALO, :]

    ext[HALO:, :] = (mm(xo[...], wo[...]) + mm(xp[...], wp[...])).astype(BF16)
    t_id = lax.broadcasted_iota(jnp.int32, (BLOCK, BLOCK + HALO), 0)
    s_id = lax.broadcasted_iota(jnp.int32, (BLOCK, BLOCK + HALO), 1)
    lag = t_id + HALO - s_id
    row_id = lax.broadcasted_iota(jnp.int32, (BLOCK, 1), 0)
    groups = mix.shape[0]
    for j in range(groups):
        window = jnp.left_shift(1, m[TP] * groups + j + 1)
        band = ((lag >= 0) & (lag < window)).astype(F32).astype(BF16)
        c = slice(j * GROUP_CH, (j + 1) * GROUP_CH)
        for b in range(rows // BLOCK):
            position = m[ROW0] + i * rows + b * BLOCK + row_id
            share = 1.0 / jnp.minimum(position + 1, window).astype(F32)
            sums = mm(band, ext[b * BLOCK : b * BLOCK + BLOCK + HALO, c])
            here = ext[b * BLOCK + HALO : b * BLOCK + BLOCK + HALO, c].astype(F32)
            diff = (sums * share - here).astype(BF16)
            out[b * BLOCK : (b + 1) * BLOCK, c] = (mm(diff, mix[j]) * scale[:, c]).astype(BF16)


def query_body(heads, m, xo, xp, wo, wp, rel, down, q_out, s_out):
    q = (mm(xo[...], wo[...]) + mm(xp[...], wp[...])).astype(BF16).astype(F32)
    up = (jax.nn.silu(q) * jnp.exp(rel[...])).astype(BF16)
    q_out[...] = up
    t_id = lax.broadcasted_iota(jnp.int32, (BLOCK, BLOCK), 0)
    s_id = lax.broadcasted_iota(jnp.int32, (BLOCK, BLOCK), 1)
    keep = t_id >= s_id
    for b in range(up.shape[0] // BLOCK):
        r = slice(b * BLOCK, (b + 1) * BLOCK)
        for h in range(heads):
            c = slice(h * DK, (h + 1) * DK)
            score = mm_t(up[r, c], down[r, c], 1, 1)
            s_out[r, c] = jnp.where(keep, score, 0.0).astype(BF16)


def gate_body(m, xo, xp, wo, wp, out):
    out[...] = (mm(xo[...], wo[...]) + mm(xp[...], wp[...])).astype(BF16)


def rec_body(heads, m, scores, up, v, gate, st, cfac, pre, recv, gain, out):
    width = heads * DK
    early = m[EARLY + 3] == 1
    factor = jnp.where(early, 1.0, 0.0)
    rows = up.shape[0]
    first = pl.program_id(0) * (rows // BLOCK)
    for h in range(heads):
        c = slice(h * DK, (h + 1) * DK)
        coming = pre[c, :] + (pre[width + h : width + h + 1, :] * factor) * recv[c, :].astype(F32)
        for b in range(rows // BLOCK):
            r = slice(b * BLOCK, (b + 1) * BLOCK)
            base = b * width + h * DK
            scale = cfac[pl.ds(first + b, 1), :][:, c]
            full = (st[base : base + DK, :].astype(F32) + scale * coming).astype(BF16)
            raw = mm(scores[r, c], v[r, c]) + mm_t(up[r, c], full, 1, 1)
            mean = jnp.mean(raw * raw, axis=-1, keepdims=True)
            g = gate[r, c].astype(F32)
            out[r, c] = (raw * lax.rsqrt(mean + EPS_RMS) * gain[...] * jax.nn.silu(g)).astype(BF16)


def pool_proj_body(m, x, po, pp, wo, wp, out):
    out[...] = ALPHA * x[...].astype(F32) + mm(po[...], wo[...]) + mm(pp[...], wp[...])


def rec_proj_body(m, base, ro, rp, wo, wp, out, stats):
    resid = base[...] + mm(ro[...], wo[...]) + mm(rp[...], wp[...])
    out[...] = resid
    mean = jnp.mean(resid, axis=-1, keepdims=True)
    dev = resid - mean
    spread = jnp.sum(dev * dev, axis=-1, keepdims=True)
    lane = lax.broadcasted_iota(jnp.int32, (resid.shape[0], DK), 1)
    stats[...] = jnp.where(lane == 0, mean, spread)


def norm_body(m, resid, own, other, gain, bias, out):
    a, b = own[...], other[...]
    mean_a, mean_b = a[:, 0:1], b[:, 0:1]
    mean = 0.5 * (mean_a + mean_b)
    half = 0.5 * (mean_a - mean_b)
    var = (a[:, 1:2] + b[:, 1:2]) * (1.0 / D) + half * half
    out[...] = ((resid[...] - mean) * lax.rsqrt(var + EPS_NORM) * gain[...] + bias[...]).astype(BF16)


def shape(rows, cols, dtype):
    return jax.ShapeDtypeStruct((rows, cols), dtype)


def local(
    stream,
    w_pool_in,
    w_query,
    w_forget,
    w_value,
    w_outgate,
    pool_mix,
    pool_scale,
    lower_bound,
    extra_decay,
    rec_gain,
    w_out_pool,
    w_out_rec,
    norm_gain,
    norm_bias,
):
    xo = stream[0]
    length, half = xo.shape
    width = lower_bound.shape[0]
    heads = width // DK
    blocks = length // BLOCK
    pool_width = w_pool_in.shape[1]
    tile = 256
    steps = length // tile
    per_tile = tile // BLOCK
    sp_n = lax.axis_size(SP)
    z, x, k = lax.axis_index("sp_0"), lax.axis_index("sp_1"), lax.axis_index("tp")
    meta = jnp.stack([k, lax.axis_index(SP) * length, x % 2, x // 2, z % 2, z // 2, k, k]).astype(jnp.int32)
    swap = [(0, 1), (1, 0)]
    pairs = [(0, 1), (1, 0), (2, 3), (3, 2)]
    mirror = [(0, 3), (3, 0), (1, 2), (2, 1)]

    xp = lax.ppermute(xo, "tp", swap)
    tail_o = lax.ppermute(xo[length - HALO :], SP, [(i, i + 1) for i in range(sp_n - 1)])
    tail_p = lax.ppermute(tail_o, "tp", swap)

    full_flops = 2 * length * D * width
    f_part, v_part = call(
        partial_body,
        meta,
        (xo, w_forget, w_value),
        [rows_spec(tile, half), own_rows(half, width), own_rows(half, width)],
        [rows_spec(tile, width)] * 2,
        [shape(length, width, F32)] * 2,
        (steps,),
        flops=full_flops,
    )
    state_rows = blocks * width
    v, down, rel, st, cfac, pay, own = call(
        functools.partial(gates_body, heads),
        meta,
        (xp, w_forget, w_value, f_part, v_part, lower_bound.reshape(1, width), extra_decay),
        [
            rows_spec(tile, half),
            other_rows(half, width),
            other_rows(half, width),
            rows_spec(tile, width),
            rows_spec(tile, width),
            whole((1, width)),
            rows_spec(tile, heads),
        ],
        [
            rows_spec(tile, width),
            rows_spec(tile, width),
            rows_spec(tile, width),
            rows_spec(per_tile * width, DK),
            whole((blocks, width)),
            whole((width + 16, DK)),
            whole((width + 8, DK)),
        ],
        [
            shape(length, width, BF16),
            shape(length, width, BF16),
            shape(length, width, F32),
            shape(state_rows, DK, BF16),
            shape(blocks, width, F32),
            shape(width + 16, DK, BF16),
            shape(width + 8, DK, F32),
        ],
        (steps,),
        scratch=[pltpu.VMEM((width, DK), F32), pltpu.VMEM((1, width), F32)],
        vmem=24,
        flops=full_flops,
    )
    pre = jnp.concatenate([jnp.zeros((width, DK), F32), jnp.ones((8, DK), F32)], axis=0)

    def combine(which, own, pre, recv):
        return call(
            functools.partial(combine_body, heads, which),
            meta,
            (own, pre, recv),
            [whole((width + 8, DK)), whole((width + 8, DK)), whole((width + 16, DK))],
            [whole((width + 16, DK)), whole((width + 8, DK)), whole((width + 8, DK))],
            [shape(width + 16, DK, BF16), shape(width + 8, DK, F32), shape(width + 8, DK, F32)],
            (1,),
            vmem=4,
            flops=width * DK * 8,
        )

    halves = [rows_spec(tile, half), rows_spec(tile, half)]
    full_w = lambda cols: [own_rows(half, cols), other_rows(half, cols)]

    got1 = lax.ppermute(pay, "sp_1", pairs)
    xo1, got1b = lax.optimization_barrier((xo, pay))
    pool_o = call(
        pool_body,
        meta,
        (xo1, xp, tail_o, tail_p, w_pool_in, w_pool_in, pool_mix, pool_scale.reshape(1, pool_width)),
        halves
        + [whole((HALO, half))] * 2
        + full_w(pool_width)
        + [whole(pool_mix.shape), whole((1, pool_width))],
        rows_spec(tile, pool_width),
        shape(length, pool_width, BF16),
        (steps,),
        scratch=[pltpu.VMEM((tile + HALO, pool_width), BF16)],
        flops=full_flops,
    )
    pool_p = lax.ppermute(pool_o, "tp", swap)
    got1, pool_o1 = lax.optimization_barrier((got1, pool_o))
    pay2, own2, pre2 = combine(0, own, pre, got1)

    got2 = lax.ppermute(pay2, "sp_1", mirror)
    rel1, _ = lax.optimization_barrier((rel, pay2))
    up, scores = call(
        functools.partial(query_body, heads),
        meta,
        (xo, xp, w_query, w_query, rel1, down),
        halves + full_w(width) + [rows_spec(tile, width)] * 2,
        [rows_spec(tile, width)] * 2,
        [shape(length, width, BF16)] * 2,
        (steps,),
        flops=full_flops,
    )
    got2, up1 = lax.optimization_barrier((got2, up))
    pay3, own3, pre3 = combine(1, own2, pre2, got2)

    got3 = lax.ppermute(pay3, "sp_0", pairs)
    xo2, _ = lax.optimization_barrier((xo, pay3))
    gate = call(
        gate_body,
        meta,
        (xo2, xp, w_outgate, w_outgate),
        halves + full_w(width),
        rows_spec(tile, width),
        shape(length, width, BF16),
        (steps,),
        flops=full_flops,
    )
    got3, gate1 = lax.optimization_barrier((got3, gate))
    pay4, _, pre4 = combine(2, own3, pre3, got3)

    got4 = lax.ppermute(pay4, "sp_0", mirror)
    wpool_p = lax.ppermute(w_out_pool, "tp", swap)
    wrec_p = lax.ppermute(w_out_rec, "tp", swap)
    pool_o2, _ = lax.optimization_barrier((pool_o1, pay4))
    base = call(
        pool_proj_body,
        meta,
        (xo, pool_o2, pool_p, w_out_pool, wpool_p),
        [rows_spec(tile, half), rows_spec(tile, pool_width), rows_spec(tile, pool_width)]
        + [own_cols(pool_width, half)] * 2,
        rows_spec(tile, half),
        shape(length, half, F32),
        (steps,),
        flops=full_flops,
    )
    got4, base = lax.optimization_barrier((got4, base))

    parts = 2
    rows = length // parts
    per = rows // tile
    recs, others = [], []
    for part in range(parts):
        first = part * per
        rec = call(
            lambda m, sc, u, vv, g, s, cf, *rest: rec_body(heads, m, sc, u, vv, g, s, cf, *rest),
            meta,
            (
                scores,
                up1,
                v,
                gate1,
                st,
                lax.slice_in_dim(cfac, part * (blocks // parts), (part + 1) * (blocks // parts)),
                pre4,
                got4,
                rec_gain.reshape(1, DK),
            ),
            [rows_spec(tile, width, first)] * 4
            + [
                rows_spec(per_tile * width, DK, first),
                whole((blocks // parts, width)),
                whole((width + 8, DK)),
                whole((width + 16, DK)),
                whole((1, DK)),
            ],
            rows_spec(tile, width),
            shape(rows, width, BF16),
            (per,),
            flops=full_flops // 4,
        )
        recs.append(rec)
        others.append(lax.ppermute(rec, "tp", swap))
    resids, stats, stats_p = [], [], []
    for part in range(parts):
        first = part * per
        resid, stat = call(
            rec_proj_body,
            meta,
            (base, recs[part], others[part], w_out_rec, wrec_p),
            [rows_spec(tile, half, first), rows_spec(tile, width), rows_spec(tile, width)]
            + [own_cols(width, half)] * 2,
            [rows_spec(tile, half), rows_spec(tile, DK)],
            [shape(rows, half, F32), shape(rows, DK, F32)],
            (per,),
            flops=full_flops // 2,
        )
        resids.append(resid)
        stats.append(stat)
        stats_p.append(lax.ppermute(stat, "tp", swap))
    out = None
    for part in range(parts):
        first = part * per
        args = (resids[part], stats[part], stats_p[part], norm_gain.reshape(1, half), norm_bias.reshape(1, half))
        specs = [rows_spec(tile, half), rows_spec(tile, DK), rows_spec(tile, DK), whole((1, half)), whole((1, half))]
        body, aliases = norm_body, None
        if out is not None:
            body = lambda m, r, a, b, g, bb, prev, o: norm_body(m, r, a, b, g, bb, o)
            args += (out,)
            specs += [pl.BlockSpec(memory_space=pl.ANY)]
            aliases = {6: 0}
        out = call(
            body,
            meta,
            args,
            specs,
            rows_spec(tile, half, first),
            shape(length, half, BF16),
            (per,),
            flops=full_flops // 8,
            aliases=aliases,
        )
    return out[None]


def solution(mesh):
    torus = Mesh(
        mesh.devices.reshape(4, 4, mesh.shape["fs"], mesh.shape["tp"]), ("sp_0", "sp_1", "fs", "tp")
    )
    return jax.shard_map(
        local,
        mesh=torus,
        in_specs=(
            P("fs", SP, "tp"),
            P(None, "tp"),
            P(None, "tp"),
            P(None, "tp"),
            P(None, "tp"),
            P(None, "tp"),
            P("tp", None, None),
            P("tp"),
            P("tp"),
            P(SP, "tp"),
            P(),
            P("tp", None),
            P("tp", None),
            P("tp"),
            P("tp"),
        ),
        out_specs=P("fs", SP, "tp"),
        check_vma=False,
    )
```

```python
import functools

import jax
import jax.numpy as jnp
from jax import lax
from jax.experimental import pallas as pl
from jax.experimental.pallas import tpu as pltpu
from jax.sharding import Mesh
from jax.sharding import PartitionSpec as P

D = 2048
DK = 128
BLOCK = 128
MID = 63
HALO = 16
GROUP_CH = 256
SP = ("sp_0", "sp_1")
ALPHA = 2.0**0.25
EPS_RMS = 1e-06
EPS_NORM = 1e-05
F32 = jnp.float32
BF16 = jnp.bfloat16
MIB = 1 << 20

TP, ROW0, EARLY = 0, 1, 2


def mm(a, b):
    return jnp.dot(a, b, preferred_element_type=F32)


def mm_t(a, b, ca, cb):
    return lax.dot_general(a, b, (((ca,), (cb,)), ((), ())), preferred_element_type=F32)


def call(body, meta, args, in_specs, out_specs, out_shape, grid, scratch=(), vmem=20, flops=0, aliases=None):
    nbytes = sum(a.size * a.dtype.itemsize for a in args)
    return pl.pallas_call(
        body,
        grid_spec=pltpu.PrefetchScalarGridSpec(
            num_scalar_prefetch=1,
            grid=grid,
            in_specs=in_specs,
            out_specs=out_specs,
            scratch_shapes=list(scratch),
        ),
        out_shape=out_shape,
        input_output_aliases=aliases or {},
        compiler_params=pltpu.CompilerParams(
            dimension_semantics=("arbitrary",) * len(grid), vmem_limit_bytes=vmem * MIB
        ),
        cost_estimate=pl.CostEstimate(flops=flops, bytes_accessed=nbytes, transcendentals=0),
    )(meta, *args)


def rows_spec(rows, cols, first=0):
    return pl.BlockSpec((rows, cols), lambda i, m: (i + first, 0))


def whole(shape):
    return pl.BlockSpec(shape, lambda i, m: (0,) * len(shape))


def own_rows(rows, cols):
    return pl.BlockSpec((rows, cols), lambda i, m: (m[TP], 0))


def other_rows(rows, cols):
    return pl.BlockSpec((rows, cols), lambda i, m: (1 - m[TP], 0))


def side(a, b):
    return jnp.concatenate([a, b], axis=1)


def stack(a, b):
    return jnp.concatenate([a, b], axis=0)


def own_cols(m, ref, cols):
    return ref[:, pl.ds(pl.multiple_of(m[TP] * cols, cols), cols)]


def tail_body(m, x, out):
    out[...] = x[...]


def gates_body(
    heads, m, xo, xp, wfo, wfp, wv_far, lb, ed, v_out, down_out, rel_out, st_out, c_out, pay_out, own_out, state, off, wv, sem
):
    i = pl.program_id(0)
    rows = xo.shape[0]
    width = heads * DK

    load = pltpu.make_async_copy(wv_far, wv, sem)

    @pl.when(i == 0)
    def _():
        load.start()
        state[...] = jnp.zeros_like(state)
        off[...] = jnp.zeros_like(off)

    features = side(xo[...], xp[...])
    f = mm(features, stack(wfo[...], wfp[...])).astype(BF16).astype(F32)

    @pl.when(i == 0)
    def _():
        load.wait()

    half = xo.shape[1]
    wv_own = wv[pl.ds(pl.multiple_of(m[TP] * half, half), half), :]
    wv_other = wv[pl.ds(pl.multiple_of((1 - m[TP]) * half, half), half), :]
    v = mm(features, stack(wv_own, wv_other)).astype(BF16)
    v_out[...] = v
    low = lb[...]
    gap = 1.0 - low
    sig = jax.nn.sigmoid(f)
    weight = gap * (1.0 - sig)
    extra = ed[...]
    extra_hi = extra.astype(BF16).astype(F32)
    extra_rows = jnp.concatenate(
        [extra_hi, extra - extra_hi, jnp.zeros_like(extra), jnp.zeros_like(extra)], axis=0
    ).astype(BF16)
    row = lax.broadcasted_iota(jnp.int32, (4 * heads, width), 0)
    head = lax.broadcasted_iota(jnp.int32, (4 * heads, width), 1) // DK
    spread = ((row == head) | (row == head + heads)).astype(F32).astype(BF16)
    log_keep = jnp.log(low + gap * sig) + mm_t(extra_rows, spread, 0, 0)
    hi = log_keep.astype(BF16)
    lo = (log_keep - hi.astype(F32)).astype(BF16)
    t_id = lax.broadcasted_iota(jnp.int32, (BLOCK, 2 * BLOCK), 0)
    s_id = lax.broadcasted_iota(jnp.int32, (BLOCK, 2 * BLOCK), 1)
    mask = (t_id >= jnp.where(s_id >= BLOCK, s_id - BLOCK, s_id)).astype(F32).astype(BF16)
    for b in range(rows // BLOCK):
        r = slice(b * BLOCK, (b + 1) * BLOCK)
        total = mm(mask, jnp.concatenate([hi[r], lo[r]], axis=0))
        middle = total[MID : MID + 1]
        end = total[BLOCK - 1 : BLOCK]
        rel = total - middle
        rel_out[r, :] = rel
        down = weight[r] * jnp.exp(-rel)
        down_out[r, :] = down.astype(BF16)
        in_weight = (down * jnp.exp(end - middle)).astype(BF16)
        e_mid, e_end = jnp.exp(middle), jnp.exp(end)
        before = off[...]
        c_out[pl.ds(i * (rows // BLOCK) + b, 1), :] = jnp.exp(middle + before)
        off[...] = before + end
        for h in range(heads):
            c = slice(h * DK, (h + 1) * DK)
            old = state[c, :]
            st_out[b * width + h * DK : b * width + (h + 1) * DK, :] = (old * e_mid[:, c]).astype(BF16)
            state[c, :] = old * e_end[:, c] + mm_t(v[r, c], in_weight[:, c], 0, 0)

    @pl.when(i == pl.num_programs(0) - 1)
    def _():
        write_payload(heads, state[...], jnp.exp(off[...]), pay_out, own_out)


def write_payload(heads, state, decay_row, pay_out, own_out):
    width = heads * DK
    decay = jnp.concatenate(
        [decay_row[:, h * DK : (h + 1) * DK] for h in range(heads)], axis=0
    )
    pack_payload(width, state, decay, pay_out)
    own_out[:width, :] = state
    own_out[width:, :] = jnp.concatenate([decay, jnp.zeros_like(decay)], axis=0)


def pack_payload(width, state, decay, pay_out):
    hi = decay.astype(BF16).astype(F32)
    pay_out[:width, :] = state.astype(BF16)
    pay_out[width:, :] = jnp.concatenate(
        [hi, decay - hi, jnp.zeros_like(hi), jnp.zeros_like(hi)], axis=0
    ).astype(BF16)


def unpack_decay(heads, width, ref):
    rows = ref[width:, :].astype(F32)
    return rows[:heads] + rows[heads : 2 * heads]


def combine_body(heads, which, m, own, *refs):
    width = heads * DK
    if which:
        pre, recv, pay_out, pre_out = refs[:4]
        own_out = refs[4] if len(refs) > 4 else None
    else:
        recv, pay_out, pre_out, own_out = refs
    early = m[EARLY + which] == 1
    d_own = own[width : width + heads, :]
    d_pre = pre[width : width + heads, :] if which else jnp.ones((heads, DK), F32)
    d_recv = unpack_decay(heads, width, recv)
    d_all = d_own * d_recv
    new_d_pre = jnp.where(early, d_recv * d_pre, d_pre)
    pre_out[width:, :] = jnp.concatenate([new_d_pre, jnp.zeros_like(d_pre)], axis=0)
    if own_out is not None:
        own_out[width:, :] = jnp.concatenate([d_all, jnp.zeros_like(d_all)], axis=0)
    states = []
    for h in range(heads):
        c = slice(h * DK, (h + 1) * DK)
        got = recv[c, :].astype(F32)
        mine = own[c, :]
        p = pre[c, :] if which else jnp.zeros((DK, DK), F32)
        pre_out[c, :] = jnp.where(early, p + d_pre[h : h + 1] * got, p)
        new = jnp.where(early, d_own[h : h + 1] * got + mine, d_recv[h : h + 1] * mine + got)
        if own_out is not None:
            own_out[c, :] = new
        states.append(new)
    pack_payload(width, jnp.concatenate(states, axis=0), d_all, pay_out)


def pool_body(m, xo, xp, to, tp, wo, wp, mix, scale, out, ext):
    i = pl.program_id(0)
    rows = xo.shape[0]

    @pl.when(i == 0)
    def _():
        ext[:HALO, :] = mm(side(to[...], tp[...]), stack(wo[...], wp[...])).astype(BF16)

    @pl.when(i > 0)
    def _():
        ext[:HALO, :] = ext[rows : rows + HALO, :]

    ext[HALO:, :] = mm(side(xo[...], xp[...]), stack(wo[...], wp[...])).astype(BF16)
    t_id = lax.broadcasted_iota(jnp.int32, (BLOCK, BLOCK + HALO), 0)
    s_id = lax.broadcasted_iota(jnp.int32, (BLOCK, BLOCK + HALO), 1)
    lag = t_id + HALO - s_id
    row_id = lax.broadcasted_iota(jnp.int32, (BLOCK, 1), 0)
    groups = mix.shape[0]
    for j in range(groups):
        window = jnp.left_shift(1, m[TP] * groups + j + 1)
        band = ((lag >= 0) & (lag < window)).astype(F32).astype(BF16)
        c = slice(j * GROUP_CH, (j + 1) * GROUP_CH)
        for b in range(rows // BLOCK):
            position = m[ROW0] + i * rows + b * BLOCK + row_id
            share = 1.0 / jnp.minimum(position + 1, window).astype(F32)
            sums = mm(band, ext[b * BLOCK : b * BLOCK + BLOCK + HALO, c])
            here = ext[b * BLOCK + HALO : b * BLOCK + BLOCK + HALO, c].astype(F32)
            diff = (sums * share - here).astype(BF16)
            out[b * BLOCK : (b + 1) * BLOCK, c] = (mm(diff, mix[j]) * scale[:, c]).astype(BF16)


def query_body(heads, m, xo, xp, wo, wp, rel, down, q_out, s_out):
    q = mm(side(xo[...], xp[...]), stack(wo[...], wp[...])).astype(BF16).astype(F32)
    up = (jax.nn.silu(q) * jnp.exp(rel[...])).astype(BF16)
    q_out[...] = up
    t_id = lax.broadcasted_iota(jnp.int32, (BLOCK, BLOCK), 0)
    s_id = lax.broadcasted_iota(jnp.int32, (BLOCK, BLOCK), 1)
    keep = t_id >= s_id
    for b in range(up.shape[0] // BLOCK):
        r = slice(b * BLOCK, (b + 1) * BLOCK)
        for h in range(heads):
            c = slice(h * DK, (h + 1) * DK)
            score = mm_t(up[r, c], down[r, c], 1, 1)
            s_out[r, c] = jnp.where(keep, score, 0.0).astype(BF16)


def gate_body(heads, m, xo, xp, wo, wp, gain, out):
    g = mm(side(xo[...], xp[...]), stack(wo[...], wp[...])).astype(BF16).astype(F32)
    out[...] = jax.nn.silu(g) * jnp.concatenate([gain[...]] * heads, axis=1)


def rec_body(heads, start, m, scores, up, v, gate, st, cfac, pre, recv, out):
    width = heads * DK
    early = m[EARLY + 3] == 1
    factor = jnp.where(early, 1.0, 0.0)
    rows = up.shape[0]
    first = start + pl.program_id(0) * (rows // BLOCK)
    for h in range(heads):
        c = slice(h * DK, (h + 1) * DK)
        coming = pre[c, :] + (pre[width + h : width + h + 1, :] * factor) * recv[c, :].astype(F32)
        for b in range(rows // BLOCK):
            r = slice(b * BLOCK, (b + 1) * BLOCK)
            base = b * width + h * DK
            scale = cfac[pl.ds(first + b, 1), :][:, c]
            full = (st[base : base + DK, :].astype(F32) + scale * coming).astype(BF16)
            raw = mm(scores[r, c], v[r, c]) + mm_t(up[r, c], full, 1, 1)
            mean = jnp.mean(raw * raw, axis=-1, keepdims=True)
            out[r, c] = (raw * lax.rsqrt(mean + EPS_RMS) * gate[r, c]).astype(BF16)


def pool_proj_body(m, x, po, pp, wo, wp, out):
    cols = out.shape[1]
    out[...] = ALPHA * x[...].astype(F32) + mm(
        side(po[...], pp[...]), stack(own_cols(m, wo, cols), own_cols(m, wp, cols))
    )


def rec_proj_body(m, base, ro, rp, wo, wp, out, stats):
    cols = out.shape[1]
    resid = base[...] + mm(side(ro[...], rp[...]), stack(own_cols(m, wo, cols), own_cols(m, wp, cols)))
    out[...] = resid
    mean = jnp.mean(resid, axis=-1, keepdims=True)
    dev = resid - mean
    spread = jnp.sum(dev * dev, axis=-1, keepdims=True)
    lane = lax.broadcasted_iota(jnp.int32, (resid.shape[0], DK), 1)
    stats[...] = jnp.where(lane == 0, mean, spread)


def norm_body(m, resid, own, other, gain, bias, out):
    a, b = own[...], other[...]
    mean_a, mean_b = a[:, 0:1], b[:, 0:1]
    mean = 0.5 * (mean_a + mean_b)
    half = 0.5 * (mean_a - mean_b)
    var = (a[:, 1:2] + b[:, 1:2]) * (1.0 / D) + half * half
    out[...] = ((resid[...] - mean) * lax.rsqrt(var + EPS_NORM) * gain[...] + bias[...]).astype(BF16)


def last_norm_body(m, resid, own, other, gain, bias, before, out):
    norm_body(m, resid, own, other, gain, bias, out)


def shape(rows, cols, dtype):
    return jax.ShapeDtypeStruct((rows, cols), dtype)


def layer(
    stream,
    w_pool_in,
    w_query,
    w_forget,
    w_value,
    w_outgate,
    pool_mix,
    pool_scale,
    lower_bound,
    extra_decay,
    rec_gain,
    w_out_pool,
    w_out_rec,
    norm_gain,
    norm_bias,
):
    xo = stream[0]
    length, half = xo.shape
    width = lower_bound.shape[0]
    heads = width // DK
    blocks = length // BLOCK
    pool_width = w_pool_in.shape[1]
    tile_gates, tile_pool, tile_query, tile_gate, tile_base = 512, 1024, 1024, 1024, 1024
    sp_n = lax.axis_size(SP)
    z, x, k = lax.axis_index("sp_0"), lax.axis_index("sp_1"), lax.axis_index("tp")
    slot = lax.iota(jnp.int32, 8)
    meta = jnp.zeros((8,), jnp.int32)
    for at, value in enumerate((k, lax.axis_index(SP) * length, x % 2, x // 2, z % 2, z // 2)):
        meta = jnp.where(slot == at, value, meta)
    xo, meta = lax.optimization_barrier((xo, meta))
    tail = call(
        tail_body,
        meta,
        (pltpu.with_memory_space_constraint(xo, pltpu.HBM),),
        [rows_spec(HALO, half, length // HALO - 1)],
        whole((HALO, half)),
        shape(HALO, half, BF16),
        (1,),
        vmem=4,
        flops=2 * length * D * width,
    )
    swap = [(0, 1), (1, 0)]
    pairs = [(0, 1), (1, 0), (2, 3), (3, 2)]
    mirror = [(0, 3), (3, 0), (1, 2), (2, 1)]

    xp = lax.ppermute(xo, "tp", swap)
    tail_o = lax.ppermute(tail, SP, [(i, i + 1) for i in range(sp_n - 1)])
    tail_p = lax.ppermute(tail_o, "tp", swap)

    full_flops = 2 * length * D * width
    halves = lambda rows: [rows_spec(rows, half), rows_spec(rows, half)]
    full_w = lambda cols: [own_rows(half, cols), other_rows(half, cols)]
    state_rows = blocks * width
    v, down, rel, st, cfac, pay, own = call(
        functools.partial(gates_body, heads),
        meta,
        (
            xo,
            xp,
            w_forget,
            w_forget,
            pltpu.with_memory_space_constraint(w_value, pltpu.HBM),
            lower_bound.reshape(1, width),
            extra_decay.T,
        ),
        halves(tile_gates)
        + full_w(width)
        + [
            pl.BlockSpec(memory_space=pl.ANY),
            whole((1, width)),
            pl.BlockSpec((heads, tile_gates), lambda i, m: (0, i)),
        ],
        [
            rows_spec(tile_gates, width),
            rows_spec(tile_gates, width),
            rows_spec(tile_gates, width),
            rows_spec(tile_gates // BLOCK * width, DK),
            whole((blocks, width)),
            whole((width + 16, DK)),
            whole((width + 8, DK)),
        ],
        [
            shape(length, width, BF16),
            shape(length, width, BF16),
            shape(length, width, F32),
            shape(state_rows, DK, BF16),
            shape(blocks, width, F32),
            shape(width + 16, DK, BF16),
            shape(width + 8, DK, F32),
        ],
        (length // tile_gates,),
        scratch=[
            pltpu.VMEM((width, DK), F32),
            pltpu.VMEM((1, width), F32),
            pltpu.VMEM((D, width), BF16),
            pltpu.SemaphoreType.DMA,
        ],
        vmem=24,
        flops=2 * full_flops,
    )

    def combine(which, *args):
        return call(
            functools.partial(combine_body, heads, which),
            meta,
            args,
            [whole((width + 8, DK))] * (len(args) - 1) + [whole((width + 16, DK))],
            [whole((width + 16, DK))] + [whole((width + 8, DK))] * (2 - which // 2),
            [shape(width + 16, DK, BF16)] + [shape(width + 8, DK, F32)] * (2 - which // 2),
            (1,),
            vmem=4,
            flops=width * DK * 8,
        )

    got1 = lax.ppermute(pay, "sp_1", pairs)
    xo1, _ = lax.optimization_barrier((xo, pay))
    pool_o = call(
        pool_body,
        meta,
        (xo1, xp, tail_o, tail_p, w_pool_in, w_pool_in, pool_mix, pool_scale.reshape(1, pool_width)),
        halves(tile_pool)
        + [whole((HALO, half))] * 2
        + full_w(pool_width)
        + [whole(pool_mix.shape), whole((1, pool_width))],
        rows_spec(tile_pool, pool_width),
        shape(length, pool_width, BF16),
        (length // tile_pool,),
        scratch=[pltpu.VMEM((tile_pool + HALO, pool_width), BF16)],
        flops=full_flops,
    )
    pool_p = lax.ppermute(pool_o, "tp", swap)
    got1, pool_o1 = lax.optimization_barrier((got1, pool_o))
    pay2, pre2, own2 = combine(0, own, got1)

    got2 = lax.ppermute(pay2, "sp_1", mirror)
    rel1, _ = lax.optimization_barrier((rel, pay2))
    up, scores = call(
        functools.partial(query_body, heads),
        meta,
        (xo, xp, w_query, w_query, rel1, down),
        halves(tile_query) + full_w(width) + [rows_spec(tile_query, width)] * 2,
        [rows_spec(tile_query, width)] * 2,
        [shape(length, width, BF16)] * 2,
        (length // tile_query,),
        flops=full_flops,
    )
    got2, up1 = lax.optimization_barrier((got2, up))
    pay3, pre3, own3 = combine(1, own2, pre2, got2)

    got3 = lax.ppermute(pay3, "sp_0", pairs)
    xo2, _ = lax.optimization_barrier((xo, pay3))
    gate = call(
        functools.partial(gate_body, heads),
        meta,
        (xo2, xp, w_outgate, w_outgate, rec_gain.reshape(1, DK)),
        halves(tile_gate) + full_w(width) + [whole((1, DK))],
        rows_spec(tile_gate, width),
        shape(length, width, F32),
        (length // tile_gate,),
        flops=full_flops,
    )
    got3, gate1 = lax.optimization_barrier((got3, gate))
    pay4, pre4 = combine(2, own3, pre3, got3)

    got4 = lax.ppermute(pay4, "sp_0", mirror)
    wpool_p = lax.ppermute(w_out_pool, "tp", swap)
    wrec_p = lax.ppermute(w_out_rec, "tp", swap)
    pool_o2, _ = lax.optimization_barrier((pool_o1, pay4))
    base = call(
        pool_proj_body,
        meta,
        (xo, pool_o2, pool_p, w_out_pool, wpool_p),
        [rows_spec(tile_base, half), rows_spec(tile_base, pool_width), rows_spec(tile_base, pool_width)]
        + [whole((pool_width, D))] * 2,
        rows_spec(tile_base, half),
        shape(length, half, F32),
        (length // tile_base,),
        flops=full_flops,
    )
    got4, base = lax.optimization_barrier((got4, base))

    parts = 2
    rows = length // parts
    tile = rows
    per_tile = tile // BLOCK
    per = rows // tile
    recs, others = [], []
    for part in range(parts):
        first = part * per
        rec = call(
            functools.partial(rec_body, heads, part * (blocks // parts)),
            meta,
            (
                scores,
                up1,
                v,
                gate1,
                st,
                cfac,
                pre4,
                got4,
            ),
            [rows_spec(tile, width, first)] * 4
            + [
                rows_spec(per_tile * width, DK, first),
                whole((blocks, width)),
                whole((width + 8, DK)),
                whole((width + 16, DK)),
            ],
            rows_spec(tile, width),
            shape(rows, width, BF16),
            (per,),
            flops=full_flops // 4,
        )
        recs.append(rec)
        others.append(lax.ppermute(rec, "tp", swap))
    gain, bias = norm_gain.reshape(1, half), norm_bias.reshape(1, half)
    base_specs = lambda first: (
        [rows_spec(tile, half, first), rows_spec(tile, width), rows_spec(tile, width)]
        + [whole((width, D))] * 2
    )
    row_specs = [rows_spec(tile, half), rows_spec(tile, DK)]
    row_shapes = [shape(rows, half, F32), shape(rows, DK, F32)]
    resid0, stat0 = call(
        rec_proj_body,
        meta,
        (base, recs[0], others[0], w_out_rec, wrec_p),
        base_specs(0),
        row_specs,
        row_shapes,
        (per,),
        flops=full_flops // 2,
    )
    stat0_p = lax.ppermute(stat0, "tp", swap)
    resid1, stat1 = call(
        rec_proj_body,
        meta,
        (base, recs[1], others[1], w_out_rec, wrec_p),
        base_specs(per),
        row_specs,
        row_shapes,
        (per,),
        flops=full_flops // 2,
    )
    stat1_p = lax.ppermute(stat1, "tp", swap)
    resid0, _ = lax.optimization_barrier((resid0, stat1))
    fine = rows // 2
    norm_specs = [rows_spec(fine, half), rows_spec(fine, DK), rows_spec(fine, DK)] + [whole((1, half))] * 2
    out = call(
        norm_body,
        meta,
        (resid0, stat0, stat0_p, gain, bias),
        norm_specs,
        rows_spec(fine, half),
        shape(length, half, BF16),
        (rows // fine,),
        flops=full_flops // 4,
    )
    out = call(
        last_norm_body,
        meta,
        (resid1, stat1, stat1_p, gain, bias, out),
        norm_specs + [pl.BlockSpec(memory_space=pl.ANY)],
        rows_spec(fine, half, rows // fine),
        shape(length, half, BF16),
        (rows // fine,),
        flops=full_flops // 4,
        aliases={6: 0},
    )
    return out[None]


def solution(mesh):
    torus = Mesh(
        mesh.devices.reshape(4, 4, mesh.shape["fs"], mesh.shape["tp"]), ("sp_0", "sp_1", "fs", "tp")
    )
    return jax.shard_map(
        layer,
        mesh=torus,
        in_specs=(
            P("fs", SP, "tp"),
            P(None, "tp"),
            P(None, "tp"),
            P(None, "tp"),
            P(None, "tp"),
            P(None, "tp"),
            P("tp", None, None),
            P("tp"),
            P("tp"),
            P(SP, "tp"),
            P(),
            P("tp", None),
            P("tp", None),
            P("tp"),
            P("tp"),
        ),
        out_specs=P("fs", SP, "tp"),
        check_vma=False,
    )
```

```python
import functools

import jax
import jax.numpy as jnp
from jax import lax
from jax.experimental import pallas as pl
from jax.experimental.pallas import tpu as pltpu
from jax.sharding import Mesh
from jax.sharding import PartitionSpec as P

D = 2048
DK = 128
BLOCK = 128
MID = 63
HALO = 16
GROUP_CH = 256
SP = ("sp_0", "sp_1")
ALPHA = 2.0**0.25
EPS_RMS = 1e-06
EPS_NORM = 1e-05
F32 = jnp.float32
BF16 = jnp.bfloat16
MIB = 1 << 20


def mm(a, b):
    return jnp.dot(a, b, preferred_element_type=F32)


def mm_t(a, b, ca, cb):
    return lax.dot_general(a, b, (((ca,), (cb,)), ((), ())), preferred_element_type=F32)


def call(body, args, in_specs, out_specs, out_shape, grid, scratch=(), vmem=20, flops=0, aliases=None):
    nbytes = sum(a.size * a.dtype.itemsize for a in args)
    return pl.pallas_call(
        body,
        grid=grid,
        in_specs=in_specs,
        out_specs=out_specs,
        scratch_shapes=list(scratch),
        out_shape=out_shape,
        input_output_aliases=aliases or {},
        compiler_params=pltpu.CompilerParams(
            dimension_semantics=("arbitrary",) * len(grid), vmem_limit_bytes=vmem * MIB
        ),
        cost_estimate=pl.CostEstimate(flops=flops, bytes_accessed=nbytes, transcendentals=0),
    )(*args)


def rows_spec(rows, cols, first=0):
    return pl.BlockSpec((rows, cols), lambda i: (i + first, 0))


def whole(shape):
    return pl.BlockSpec(shape, lambda i: (0,) * len(shape))


def side(a, b):
    return jnp.concatenate([a, b], axis=1)


def stack(a, b):
    return jnp.concatenate([a, b], axis=0)


def own_cols(ref, cols):
    return ref[:, pl.ds(pl.multiple_of(lax.axis_index("tp") * cols, cols), cols)]


def own_then_other(ref):
    half = ref.shape[0] // 2
    k = lax.axis_index("tp")
    return stack(
        ref[pl.ds(pl.multiple_of(k * half, half), half), :],
        ref[pl.ds(pl.multiple_of((1 - k) * half, half), half), :],
    )


def later(which):
    place = lax.axis_index("sp_1" if which < 2 else "sp_0")
    return (place % 2 if which % 2 == 0 else place // 2) == 1


def tail_body(x, out):
    out[...] = x[...]


def gates_body(
    heads, xo, xp, wf, wv_far, lb, ed, v_out, down_out, rel_out, st_out, c_out, pay_out, own_out, state, off, wv, sem
):
    i = pl.program_id(0)
    rows = xo.shape[0]
    width = heads * DK

    load = pltpu.make_async_copy(wv_far, wv, sem)

    @pl.when(i == 0)
    def _():
        load.start()
        state[...] = jnp.zeros_like(state)
        off[...] = jnp.zeros_like(off)

    features = side(xo[...], xp[...])
    f = mm(features, own_then_other(wf)).astype(BF16).astype(F32)

    @pl.when(i == 0)
    def _():
        load.wait()

    v = mm(features, own_then_other(wv)).astype(BF16)
    v_out[...] = v
    low = lb[...]
    gap = 1.0 - low
    sig = jax.nn.sigmoid(f)
    weight = gap * (1.0 - sig)
    extra = ed[...]
    extra_hi = extra.astype(BF16).astype(F32)
    extra_rows = jnp.concatenate(
        [extra_hi, extra - extra_hi, jnp.zeros_like(extra), jnp.zeros_like(extra)], axis=0
    ).astype(BF16)
    row = lax.broadcasted_iota(jnp.int32, (4 * heads, width), 0)
    head = lax.broadcasted_iota(jnp.int32, (4 * heads, width), 1) // DK
    spread = ((row == head) | (row == head + heads)).astype(F32).astype(BF16)
    log_keep = jnp.log(low + gap * sig) + mm_t(extra_rows, spread, 0, 0)
    hi = log_keep.astype(BF16)
    lo = (log_keep - hi.astype(F32)).astype(BF16)
    t_id = lax.broadcasted_iota(jnp.int32, (BLOCK, 2 * BLOCK), 0)
    s_id = lax.broadcasted_iota(jnp.int32, (BLOCK, 2 * BLOCK), 1)
    mask = (t_id >= jnp.where(s_id >= BLOCK, s_id - BLOCK, s_id)).astype(F32).astype(BF16)
    for b in range(rows // BLOCK):
        r = slice(b * BLOCK, (b + 1) * BLOCK)
        total = mm(mask, jnp.concatenate([hi[r], lo[r]], axis=0))
        middle = total[MID : MID + 1]
        end = total[BLOCK - 1 : BLOCK]
        rel = total - middle
        rel_out[r, :] = rel
        down = weight[r] * jnp.exp(-rel)
        down_out[r, :] = down.astype(BF16)
        in_weight = (down * jnp.exp(end - middle)).astype(BF16)
        e_mid, e_end = jnp.exp(middle), jnp.exp(end)
        before = off[...]
        c_out[pl.ds(i * (rows // BLOCK) + b, 1), :] = jnp.exp(middle + before)
        off[...] = before + end
        for h in range(heads):
            c = slice(h * DK, (h + 1) * DK)
            old = state[c, :]
            st_out[b * width + h * DK : b * width + (h + 1) * DK, :] = (old * e_mid[:, c]).astype(BF16)
            state[c, :] = old * e_end[:, c] + mm_t(v[r, c], in_weight[:, c], 0, 0)

    @pl.when(i == pl.num_programs(0) - 1)
    def _():
        write_payload(heads, state[...], jnp.exp(off[...]), pay_out, own_out)


def write_payload(heads, state, decay_row, pay_out, own_out):
    width = heads * DK
    decay = jnp.concatenate(
        [decay_row[:, h * DK : (h + 1) * DK] for h in range(heads)], axis=0
    )
    pack_payload(width, state, decay, pay_out)
    own_out[:width, :] = state
    own_out[width:, :] = jnp.concatenate([decay, jnp.zeros_like(decay)], axis=0)


def pack_payload(width, state, decay, pay_out):
    hi = decay.astype(BF16).astype(F32)
    pay_out[:width, :] = state.astype(BF16)
    pay_out[width:, :] = jnp.concatenate(
        [hi, decay - hi, jnp.zeros_like(hi), jnp.zeros_like(hi)], axis=0
    ).astype(BF16)


def unpack_decay(heads, width, ref):
    rows = ref[width:, :].astype(F32)
    return rows[:heads] + rows[heads : 2 * heads]


def combine_body(heads, which, own, *refs):
    width = heads * DK
    if which:
        pre, recv, pay_out, pre_out = refs[:4]
        own_out = refs[4] if len(refs) > 4 else None
    else:
        recv, pay_out, pre_out, own_out = refs
    early = later(which)
    d_own = own[width : width + heads, :]
    d_pre = pre[width : width + heads, :] if which else jnp.ones((heads, DK), F32)
    d_recv = unpack_decay(heads, width, recv)
    d_all = d_own * d_recv
    new_d_pre = jnp.where(early, d_recv * d_pre, d_pre)
    pre_out[width:, :] = jnp.concatenate([new_d_pre, jnp.zeros_like(d_pre)], axis=0)
    if own_out is not None:
        own_out[width:, :] = jnp.concatenate([d_all, jnp.zeros_like(d_all)], axis=0)
    states = []
    for h in range(heads):
        c = slice(h * DK, (h + 1) * DK)
        got = recv[c, :].astype(F32)
        mine = own[c, :]
        p = pre[c, :] if which else jnp.zeros((DK, DK), F32)
        pre_out[c, :] = jnp.where(early, p + d_pre[h : h + 1] * got, p)
        new = jnp.where(early, d_own[h : h + 1] * got + mine, d_recv[h : h + 1] * mine + got)
        if own_out is not None:
            own_out[c, :] = new
        states.append(new)
    pack_payload(width, jnp.concatenate(states, axis=0), d_all, pay_out)


def pool_body(length, xo, xp, to, tp, w, mix, scale, out, ext):
    i = pl.program_id(0)
    rows = xo.shape[0]

    @pl.when(i == 0)
    def _():
        ext[:HALO, :] = mm(side(to[...], tp[...]), own_then_other(w)).astype(BF16)

    @pl.when(i > 0)
    def _():
        ext[:HALO, :] = ext[rows : rows + HALO, :]

    ext[HALO:, :] = mm(side(xo[...], xp[...]), own_then_other(w)).astype(BF16)
    t_id = lax.broadcasted_iota(jnp.int32, (BLOCK, BLOCK + HALO), 0)
    s_id = lax.broadcasted_iota(jnp.int32, (BLOCK, BLOCK + HALO), 1)
    lag = t_id + HALO - s_id
    row_id = lax.broadcasted_iota(jnp.int32, (BLOCK, 1), 0)
    groups = mix.shape[0]
    for j in range(groups):
        window = jnp.left_shift(1, lax.axis_index("tp") * groups + j + 1)
        band = ((lag >= 0) & (lag < window)).astype(F32).astype(BF16)
        c = slice(j * GROUP_CH, (j + 1) * GROUP_CH)
        for b in range(rows // BLOCK):
            position = lax.axis_index(SP) * length + i * rows + b * BLOCK + row_id
            share = 1.0 / jnp.minimum(position + 1, window).astype(F32)
            sums = mm(band, ext[b * BLOCK : b * BLOCK + BLOCK + HALO, c])
            here = ext[b * BLOCK + HALO : b * BLOCK + BLOCK + HALO, c].astype(F32)
            diff = (sums * share - here).astype(BF16)
            out[b * BLOCK : (b + 1) * BLOCK, c] = (mm(diff, mix[j]) * scale[:, c]).astype(BF16)


def query_body(heads, xo, xp, w, rel, down, q_out, s_out):
    q = mm(side(xo[...], xp[...]), own_then_other(w)).astype(BF16).astype(F32)
    up = (jax.nn.silu(q) * jnp.exp(rel[...])).astype(BF16)
    q_out[...] = up
    t_id = lax.broadcasted_iota(jnp.int32, (BLOCK, BLOCK), 0)
    s_id = lax.broadcasted_iota(jnp.int32, (BLOCK, BLOCK), 1)
    keep = t_id >= s_id
    for b in range(up.shape[0] // BLOCK):
        r = slice(b * BLOCK, (b + 1) * BLOCK)
        for h in range(heads):
            c = slice(h * DK, (h + 1) * DK)
            score = mm_t(up[r, c], down[r, c], 1, 1)
            s_out[r, c] = jnp.where(keep, score, 0.0).astype(BF16)


def gate_body(heads, xo, xp, w, gain, out):
    g = mm(side(xo[...], xp[...]), own_then_other(w)).astype(BF16).astype(F32)
    out[...] = jax.nn.silu(g) * jnp.concatenate([gain[...]] * heads, axis=1)


def rec_body(heads, start, scores, up, v, gate, st, cfac, pre, recv, out):
    width = heads * DK
    early = later(3)
    factor = jnp.where(early, 1.0, 0.0)
    rows = up.shape[0]
    first = start + pl.program_id(0) * (rows // BLOCK)
    for h in range(heads):
        c = slice(h * DK, (h + 1) * DK)
        coming = pre[c, :] + (pre[width + h : width + h + 1, :] * factor) * recv[c, :].astype(F32)
        for b in range(rows // BLOCK):
            r = slice(b * BLOCK, (b + 1) * BLOCK)
            base = b * width + h * DK
            scale = cfac[pl.ds(first + b, 1), :][:, c]
            full = (st[base : base + DK, :].astype(F32) + scale * coming).astype(BF16)
            raw = mm(scores[r, c], v[r, c]) + mm_t(up[r, c], full, 1, 1)
            mean = jnp.mean(raw * raw, axis=-1, keepdims=True)
            out[r, c] = (raw * lax.rsqrt(mean + EPS_RMS) * gate[r, c]).astype(BF16)


def pool_proj_body(x, po, pp, wo, wp, out):
    cols = out.shape[1]
    out[...] = ALPHA * x[...].astype(F32) + mm(
        side(po[...], pp[...]), stack(own_cols(wo, cols), own_cols(wp, cols))
    )


def rec_proj_body(base, ro, rp, wo, wp, out, stats):
    cols = out.shape[1]
    resid = base[...] + mm(side(ro[...], rp[...]), stack(own_cols(wo, cols), own_cols(wp, cols)))
    out[...] = resid
    mean = jnp.mean(resid, axis=-1, keepdims=True)
    dev = resid - mean
    spread = jnp.sum(dev * dev, axis=-1, keepdims=True)
    lane = lax.broadcasted_iota(jnp.int32, (resid.shape[0], DK), 1)
    stats[...] = jnp.where(lane == 0, mean, spread)


def norm_body(resid, own, other, gain, bias, out):
    a, b = own[...], other[...]
    mean_a, mean_b = a[:, 0:1], b[:, 0:1]
    mean = 0.5 * (mean_a + mean_b)
    half = 0.5 * (mean_a - mean_b)
    var = (a[:, 1:2] + b[:, 1:2]) * (1.0 / D) + half * half
    out[...] = ((resid[...] - mean) * lax.rsqrt(var + EPS_NORM) * gain[...] + bias[...]).astype(BF16)


def last_norm_body(resid, own, other, gain, bias, before, out):
    norm_body(resid, own, other, gain, bias, out)


def shape(rows, cols, dtype):
    return jax.ShapeDtypeStruct((rows, cols), dtype)


def layer(
    stream,
    w_pool_in,
    w_query,
    w_forget,
    w_value,
    w_outgate,
    pool_mix,
    pool_scale,
    lower_bound,
    extra_decay,
    rec_gain,
    w_out_pool,
    w_out_rec,
    norm_gain,
    norm_bias,
):
    xo = stream[0]
    length, half = xo.shape
    width = lower_bound.shape[0]
    heads = width // DK
    blocks = length // BLOCK
    pool_width = w_pool_in.shape[1]
    tile_gates, tile_pool, tile_query, tile_gate, tile_base = 512, 1024, 1024, 1024, 1024
    sp_n = lax.axis_size(SP)
    tail = call(
        tail_body,
        (pltpu.with_memory_space_constraint(xo, pltpu.HBM),),
        [rows_spec(HALO, half, length // HALO - 1)],
        whole((HALO, half)),
        shape(HALO, half, BF16),
        (1,),
        vmem=4,
        flops=2 * length * D * width,
    )
    swap = [(0, 1), (1, 0)]
    pairs = [(0, 1), (1, 0), (2, 3), (3, 2)]
    mirror = [(0, 3), (3, 0), (1, 2), (2, 1)]

    xp = lax.ppermute(xo, "tp", swap)
    tail_o = lax.ppermute(tail, SP, [(i, i + 1) for i in range(sp_n - 1)])
    tail_p = lax.ppermute(tail_o, "tp", swap)

    full_flops = 2 * length * D * width
    halves = lambda rows: [rows_spec(rows, half), rows_spec(rows, half)]
    full_w = lambda cols: [whole((D, cols))]
    state_rows = blocks * width
    v, down, rel, st, cfac, pay, own = call(
        functools.partial(gates_body, heads),
        (
            xo,
            xp,
            w_forget,
            pltpu.with_memory_space_constraint(w_value, pltpu.HBM),
            lower_bound.reshape(1, width),
            extra_decay.T,
        ),
        halves(tile_gates)
        + full_w(width)
        + [
            pl.BlockSpec(memory_space=pl.ANY),
            whole((1, width)),
            pl.BlockSpec((heads, tile_gates), lambda i: (0, i)),
        ],
        [
            rows_spec(tile_gates, width),
            rows_spec(tile_gates, width),
            rows_spec(tile_gates, width),
            rows_spec(tile_gates // BLOCK * width, DK),
            whole((blocks, width)),
            whole((width + 16, DK)),
            whole((width + 8, DK)),
        ],
        [
            shape(length, width, BF16),
            shape(length, width, BF16),
            shape(length, width, F32),
            shape(state_rows, DK, BF16),
            shape(blocks, width, F32),
            shape(width + 16, DK, BF16),
            shape(width + 8, DK, F32),
        ],
        (length // tile_gates,),
        scratch=[
            pltpu.VMEM((width, DK), F32),
            pltpu.VMEM((1, width), F32),
            pltpu.VMEM((D, width), BF16),
            pltpu.SemaphoreType.DMA,
        ],
        vmem=24,
        flops=2 * full_flops,
    )

    def combine(which, *args):
        return call(
            functools.partial(combine_body, heads, which),
                args,
            [whole((width + 8, DK))] * (len(args) - 1) + [whole((width + 16, DK))],
            [whole((width + 16, DK))] + [whole((width + 8, DK))] * (2 - which // 2),
            [shape(width + 16, DK, BF16)] + [shape(width + 8, DK, F32)] * (2 - which // 2),
            (1,),
            vmem=4,
            flops=width * DK * 8,
        )

    got1 = lax.ppermute(pay, "sp_1", pairs)
    xo1, _ = lax.optimization_barrier((xo, pay))
    pool_o = call(
        functools.partial(pool_body, length),
        (xo1, xp, tail_o, tail_p, w_pool_in, pool_mix, pool_scale.reshape(1, pool_width)),
        halves(tile_pool)
        + [whole((HALO, half))] * 2
        + full_w(pool_width)
        + [whole(pool_mix.shape), whole((1, pool_width))],
        rows_spec(tile_pool, pool_width),
        shape(length, pool_width, BF16),
        (length // tile_pool,),
        scratch=[pltpu.VMEM((tile_pool + HALO, pool_width), BF16)],
        flops=full_flops,
    )
    pool_p = lax.ppermute(pool_o, "tp", swap)
    got1, pool_o1 = lax.optimization_barrier((got1, pool_o))
    pay2, pre2, own2 = combine(0, own, got1)

    got2 = lax.ppermute(pay2, "sp_1", mirror)
    rel1, _ = lax.optimization_barrier((rel, pay2))
    up, scores = call(
        functools.partial(query_body, heads),
        (xo, xp, w_query, rel1, down),
        halves(tile_query) + full_w(width) + [rows_spec(tile_query, width)] * 2,
        [rows_spec(tile_query, width)] * 2,
        [shape(length, width, BF16)] * 2,
        (length // tile_query,),
        flops=full_flops,
    )
    got2, up1 = lax.optimization_barrier((got2, up))
    pay3, pre3, own3 = combine(1, own2, pre2, got2)

    got3 = lax.ppermute(pay3, "sp_0", pairs)
    xo2, _ = lax.optimization_barrier((xo, pay3))
    gate = call(
        functools.partial(gate_body, heads),
        (xo2, xp, w_outgate, rec_gain.reshape(1, DK)),
        halves(tile_gate) + full_w(width) + [whole((1, DK))],
        rows_spec(tile_gate, width),
        shape(length, width, F32),
        (length // tile_gate,),
        flops=full_flops,
    )
    got3, gate1 = lax.optimization_barrier((got3, gate))
    pay4, pre4 = combine(2, own3, pre3, got3)

    got4 = lax.ppermute(pay4, "sp_0", mirror)
    wpool_p = lax.ppermute(w_out_pool, "tp", swap)
    wrec_p = lax.ppermute(w_out_rec, "tp", swap)
    pool_o2, _ = lax.optimization_barrier((pool_o1, pay4))
    base = call(
        pool_proj_body,
        (xo, pool_o2, pool_p, w_out_pool, wpool_p),
        [rows_spec(tile_base, half), rows_spec(tile_base, pool_width), rows_spec(tile_base, pool_width)]
        + [whole((pool_width, D))] * 2,
        rows_spec(tile_base, half),
        shape(length, half, F32),
        (length // tile_base,),
        flops=full_flops,
    )
    got4, base = lax.optimization_barrier((got4, base))

    parts = 2
    rows = length // parts
    tile = rows
    per_tile = tile // BLOCK
    per = rows // tile
    recs, others = [], []
    for part in range(parts):
        first = part * per
        rec = call(
            functools.partial(rec_body, heads, part * (blocks // parts)),
                (
                scores,
                up1,
                v,
                gate1,
                st,
                cfac,
                pre4,
                got4,
            ),
            [rows_spec(tile, width, first)] * 4
            + [
                rows_spec(per_tile * width, DK, first),
                whole((blocks, width)),
                whole((width + 8, DK)),
                whole((width + 16, DK)),
            ],
            rows_spec(tile, width),
            shape(rows, width, BF16),
            (per,),
            flops=full_flops // 4,
        )
        recs.append(rec)
        others.append(lax.ppermute(rec, "tp", swap))
    gain, bias = norm_gain.reshape(1, half), norm_bias.reshape(1, half)
    base_specs = lambda first: (
        [rows_spec(tile, half, first), rows_spec(tile, width), rows_spec(tile, width)]
        + [whole((width, D))] * 2
    )
    row_specs = [rows_spec(tile, half), rows_spec(tile, DK)]
    row_shapes = [shape(rows, half, F32), shape(rows, DK, F32)]
    resid0, stat0 = call(
        rec_proj_body,
        (base, recs[0], others[0], w_out_rec, wrec_p),
        base_specs(0),
        row_specs,
        row_shapes,
        (per,),
        flops=full_flops // 2,
    )
    stat0_p = lax.ppermute(stat0, "tp", swap)
    resid1, stat1 = call(
        rec_proj_body,
        (base, recs[1], others[1], w_out_rec, wrec_p),
        base_specs(per),
        row_specs,
        row_shapes,
        (per,),
        flops=full_flops // 2,
    )
    stat1_p = lax.ppermute(stat1, "tp", swap)
    resid0, _ = lax.optimization_barrier((resid0, stat1))
    fine = rows // 2
    norm_specs = [rows_spec(fine, half), rows_spec(fine, DK), rows_spec(fine, DK)] + [whole((1, half))] * 2
    out = call(
        norm_body,
        (resid0, stat0, stat0_p, gain, bias),
        norm_specs,
        rows_spec(fine, half),
        shape(length, half, BF16),
        (rows // fine,),
        flops=full_flops // 4,
    )
    out = call(
        last_norm_body,
        (resid1, stat1, stat1_p, gain, bias, out),
        norm_specs + [pl.BlockSpec(memory_space=pl.ANY)],
        rows_spec(fine, half, rows // fine),
        shape(length, half, BF16),
        (rows // fine,),
        flops=full_flops // 4,
        aliases={5: 0},
    )
    return out[None]


def solution(mesh):
    torus = Mesh(
        mesh.devices.reshape(4, 4, mesh.shape["fs"], mesh.shape["tp"]), ("sp_0", "sp_1", "fs", "tp")
    )
    return jax.shard_map(
        layer,
        mesh=torus,
        in_specs=(
            P("fs", SP, "tp"),
            P(None, "tp"),
            P(None, "tp"),
            P(None, "tp"),
            P(None, "tp"),
            P(None, "tp"),
            P("tp", None, None),
            P("tp"),
            P("tp"),
            P(SP, "tp"),
            P(),
            P("tp", None),
            P("tp", None),
            P("tp"),
            P("tp"),
        ),
        out_specs=P("fs", SP, "tp"),
        check_vma=False,
    )
```

```python
import functools

import jax
import jax.numpy as jnp
from jax import lax
from jax.experimental import pallas as pl
from jax.experimental.pallas import tpu as pltpu
from jax.sharding import Mesh
from jax.sharding import PartitionSpec as P

D = 2048
DK = 128
BLOCK = 128
MID = 63
HALO = 16
GROUP_CH = 256
SP = ("sp_0", "sp_1")
ALPHA = 2.0**0.25
EPS_RMS = 1e-06
EPS_NORM = 1e-05
F32 = jnp.float32
BF16 = jnp.bfloat16
MIB = 1 << 20


def mm(a, b):
    return jnp.dot(a, b, preferred_element_type=F32)


def mm_t(a, b, ca, cb):
    return lax.dot_general(a, b, (((ca,), (cb,)), ((), ())), preferred_element_type=F32)


def call(body, args, in_specs, out_specs, out_shape, grid, scratch=(), vmem=20, flops=0, aliases=None):
    nbytes = sum(a.size * a.dtype.itemsize for a in args)
    return pl.pallas_call(
        body,
        grid=grid,
        in_specs=in_specs,
        out_specs=out_specs,
        scratch_shapes=list(scratch),
        out_shape=out_shape,
        input_output_aliases=aliases or {},
        compiler_params=pltpu.CompilerParams(
            dimension_semantics=("arbitrary",) * len(grid), vmem_limit_bytes=vmem * MIB
        ),
        cost_estimate=pl.CostEstimate(flops=flops, bytes_accessed=nbytes, transcendentals=0),
    )(*args)


def rows_spec(rows, cols, first=0):
    return pl.BlockSpec((rows, cols), lambda i: (i + first, 0))


def whole(shape):
    return pl.BlockSpec(shape, lambda i: (0,) * len(shape))


def side(a, b):
    return jnp.concatenate([a, b], axis=1)


def stack(a, b):
    return jnp.concatenate([a, b], axis=0)


def own_cols(ref, cols):
    return ref[:, pl.ds(pl.multiple_of(lax.axis_index("tp") * cols, cols), cols)]


def own_then_other(ref):
    half = ref.shape[0] // 2
    k = lax.axis_index("tp")
    return stack(
        ref[pl.ds(pl.multiple_of(k * half, half), half), :],
        ref[pl.ds(pl.multiple_of((1 - k) * half, half), half), :],
    )


def later(which):
    place = lax.axis_index("sp_1" if which < 2 else "sp_0")
    return (place % 2 if which % 2 == 0 else place // 2) == 1


def tail_body(x, out):
    out[...] = x[...]


def half_rows(ref, which):
    half = ref.shape[0] // 2
    return ref[pl.ds(pl.multiple_of(which * half, half), half), :]


def part_body(xo, wf, out):
    out[...] = mm(xo[...], half_rows(wf, lax.axis_index("tp")))


def value_body(xo, xp, w, out):
    out[...] = mm(side(xo[...], xp[...]), own_then_other(w)).astype(BF16)


def gates_body(heads, part, xp, wf, v, lb, ed, down_out, rel_out, st_out, c_out, pay_out, own_out, state, off):
    i = pl.program_id(0)
    rows = xp.shape[0]
    width = heads * DK

    @pl.when(i == 0)
    def _():
        state[...] = jnp.zeros_like(state)
        off[...] = jnp.zeros_like(off)

    f = (part[...] + mm(xp[...], half_rows(wf, 1 - lax.axis_index("tp")))).astype(BF16).astype(F32)
    low = lb[...]
    gap = 1.0 - low
    sig = jax.nn.sigmoid(f)
    weight = gap * (1.0 - sig)
    extra = ed[...]
    extra_hi = extra.astype(BF16).astype(F32)
    extra_rows = jnp.concatenate(
        [extra_hi, extra - extra_hi, jnp.zeros_like(extra), jnp.zeros_like(extra)], axis=0
    ).astype(BF16)
    row = lax.broadcasted_iota(jnp.int32, (4 * heads, width), 0)
    head = lax.broadcasted_iota(jnp.int32, (4 * heads, width), 1) // DK
    spread = ((row == head) | (row == head + heads)).astype(F32).astype(BF16)
    log_keep = jnp.log(low + gap * sig) + mm_t(extra_rows, spread, 0, 0)
    hi = log_keep.astype(BF16)
    lo = (log_keep - hi.astype(F32)).astype(BF16)
    t_id = lax.broadcasted_iota(jnp.int32, (BLOCK, 2 * BLOCK), 0)
    s_id = lax.broadcasted_iota(jnp.int32, (BLOCK, 2 * BLOCK), 1)
    mask = (t_id >= jnp.where(s_id >= BLOCK, s_id - BLOCK, s_id)).astype(F32).astype(BF16)
    for b in range(rows // BLOCK):
        r = slice(b * BLOCK, (b + 1) * BLOCK)
        total = mm(mask, jnp.concatenate([hi[r], lo[r]], axis=0))
        middle = total[MID : MID + 1]
        end = total[BLOCK - 1 : BLOCK]
        rel = total - middle
        rel_out[r, :] = rel
        down = weight[r] * jnp.exp(-rel)
        down_out[r, :] = down.astype(BF16)
        in_weight = (down * jnp.exp(end - middle)).astype(BF16)
        e_mid, e_end = jnp.exp(middle), jnp.exp(end)
        before = off[...]
        c_out[pl.ds(i * (rows // BLOCK) + b, 1), :] = jnp.exp(middle + before)
        off[...] = before + end
        for h in range(heads):
            c = slice(h * DK, (h + 1) * DK)
            old = state[c, :]
            st_out[b * width + h * DK : b * width + (h + 1) * DK, :] = (old * e_mid[:, c]).astype(BF16)
            state[c, :] = old * e_end[:, c] + mm_t(v[r, c], in_weight[:, c], 0, 0)

    @pl.when(i == pl.num_programs(0) - 1)
    def _():
        write_payload(heads, state[...], jnp.exp(off[...]), pay_out, own_out)


def write_payload(heads, state, decay_row, pay_out, own_out):
    width = heads * DK
    decay = jnp.concatenate(
        [decay_row[:, h * DK : (h + 1) * DK] for h in range(heads)], axis=0
    )
    pack_payload(width, state, decay, pay_out)
    own_out[:width, :] = state
    own_out[width:, :] = jnp.concatenate([decay, jnp.zeros_like(decay)], axis=0)


def pack_payload(width, state, decay, pay_out):
    hi = decay.astype(BF16).astype(F32)
    pay_out[:width, :] = state.astype(BF16)
    pay_out[width:, :] = jnp.concatenate(
        [hi, decay - hi, jnp.zeros_like(hi), jnp.zeros_like(hi)], axis=0
    ).astype(BF16)


def unpack_decay(heads, width, ref):
    rows = ref[width:, :].astype(F32)
    return rows[:heads] + rows[heads : 2 * heads]


def combine_body(heads, which, own, *refs):
    width = heads * DK
    if which:
        pre, recv, pay_out, pre_out = refs[:4]
        own_out = refs[4] if len(refs) > 4 else None
    else:
        recv, pay_out, pre_out, own_out = refs
    early = later(which)
    d_own = own[width : width + heads, :]
    d_pre = pre[width : width + heads, :] if which else jnp.ones((heads, DK), F32)
    d_recv = unpack_decay(heads, width, recv)
    d_all = d_own * d_recv
    new_d_pre = jnp.where(early, d_recv * d_pre, d_pre)
    pre_out[width:, :] = jnp.concatenate([new_d_pre, jnp.zeros_like(d_pre)], axis=0)
    if own_out is not None:
        own_out[width:, :] = jnp.concatenate([d_all, jnp.zeros_like(d_all)], axis=0)
    states = []
    for h in range(heads):
        c = slice(h * DK, (h + 1) * DK)
        got = recv[c, :].astype(F32)
        mine = own[c, :]
        p = pre[c, :] if which else jnp.zeros((DK, DK), F32)
        pre_out[c, :] = jnp.where(early, p + d_pre[h : h + 1] * got, p)
        new = jnp.where(early, d_own[h : h + 1] * got + mine, d_recv[h : h + 1] * mine + got)
        if own_out is not None:
            own_out[c, :] = new
        states.append(new)
    pack_payload(width, jnp.concatenate(states, axis=0), d_all, pay_out)


def pool_body(length, xo, xp, to, tp, w, mix, scale, out, ext):
    i = pl.program_id(0)
    rows = xo.shape[0]

    @pl.when(i == 0)
    def _():
        ext[:HALO, :] = mm(side(to[...], tp[...]), own_then_other(w)).astype(BF16)

    @pl.when(i > 0)
    def _():
        ext[:HALO, :] = ext[rows : rows + HALO, :]

    ext[HALO:, :] = mm(side(xo[...], xp[...]), own_then_other(w)).astype(BF16)
    t_id = lax.broadcasted_iota(jnp.int32, (BLOCK, BLOCK + HALO), 0)
    s_id = lax.broadcasted_iota(jnp.int32, (BLOCK, BLOCK + HALO), 1)
    lag = t_id + HALO - s_id
    row_id = lax.broadcasted_iota(jnp.int32, (BLOCK, 1), 0)
    groups = mix.shape[0]
    for j in range(groups):
        window = jnp.left_shift(1, lax.axis_index("tp") * groups + j + 1)
        band = ((lag >= 0) & (lag < window)).astype(F32).astype(BF16)
        c = slice(j * GROUP_CH, (j + 1) * GROUP_CH)
        for b in range(rows // BLOCK):
            position = lax.axis_index(SP) * length + i * rows + b * BLOCK + row_id
            share = 1.0 / jnp.minimum(position + 1, window).astype(F32)
            sums = mm(band, ext[b * BLOCK : b * BLOCK + BLOCK + HALO, c])
            here = ext[b * BLOCK + HALO : b * BLOCK + BLOCK + HALO, c].astype(F32)
            diff = (sums * share - here).astype(BF16)
            out[b * BLOCK : (b + 1) * BLOCK, c] = (mm(diff, mix[j]) * scale[:, c]).astype(BF16)


def query_body(heads, xo, xp, w, rel, down, q_out, s_out):
    q = mm(side(xo[...], xp[...]), own_then_other(w)).astype(BF16).astype(F32)
    up = (jax.nn.silu(q) * jnp.exp(rel[...])).astype(BF16)
    q_out[...] = up
    t_id = lax.broadcasted_iota(jnp.int32, (BLOCK, BLOCK), 0)
    s_id = lax.broadcasted_iota(jnp.int32, (BLOCK, BLOCK), 1)
    keep = t_id >= s_id
    for b in range(up.shape[0] // BLOCK):
        r = slice(b * BLOCK, (b + 1) * BLOCK)
        for h in range(heads):
            c = slice(h * DK, (h + 1) * DK)
            score = mm_t(up[r, c], down[r, c], 1, 1)
            s_out[r, c] = jnp.where(keep, score, 0.0).astype(BF16)


def gate_body(heads, xo, xp, w, gain, out):
    g = mm(side(xo[...], xp[...]), own_then_other(w)).astype(BF16).astype(F32)
    out[...] = jax.nn.silu(g) * jnp.concatenate([gain[...]] * heads, axis=1)


def rec_body(heads, start, scores, up, v, gate, st, cfac, pre, recv, out):
    width = heads * DK
    early = later(3)
    factor = jnp.where(early, 1.0, 0.0)
    rows = up.shape[0]
    first = start + pl.program_id(0) * (rows // BLOCK)
    for h in range(heads):
        c = slice(h * DK, (h + 1) * DK)
        coming = pre[c, :] + (pre[width + h : width + h + 1, :] * factor) * recv[c, :].astype(F32)
        for b in range(rows // BLOCK):
            r = slice(b * BLOCK, (b + 1) * BLOCK)
            base = b * width + h * DK
            scale = cfac[pl.ds(first + b, 1), :][:, c]
            full = (st[base : base + DK, :].astype(F32) + scale * coming).astype(BF16)
            raw = mm(scores[r, c], v[r, c]) + mm_t(up[r, c], full, 1, 1)
            mean = jnp.mean(raw * raw, axis=-1, keepdims=True)
            out[r, c] = (raw * lax.rsqrt(mean + EPS_RMS) * gate[r, c]).astype(BF16)


def pool_proj_body(x, po, pp, wo, wp, out):
    cols = out.shape[1]
    out[...] = ALPHA * x[...].astype(F32) + mm(
        side(po[...], pp[...]), stack(own_cols(wo, cols), own_cols(wp, cols))
    )


def rec_proj_body(base, ro, rp, wo, wp, out, stats):
    cols = out.shape[1]
    resid = base[...] + mm(side(ro[...], rp[...]), stack(own_cols(wo, cols), own_cols(wp, cols)))
    out[...] = resid
    mean = jnp.mean(resid, axis=-1, keepdims=True)
    dev = resid - mean
    spread = jnp.sum(dev * dev, axis=-1, keepdims=True)
    lane = lax.broadcasted_iota(jnp.int32, (resid.shape[0], DK), 1)
    stats[...] = jnp.where(lane == 0, mean, spread)


def norm_body(resid, own, other, gain, bias, out):
    a, b = own[...], other[...]
    mean_a, mean_b = a[:, 0:1], b[:, 0:1]
    mean = 0.5 * (mean_a + mean_b)
    half = 0.5 * (mean_a - mean_b)
    var = (a[:, 1:2] + b[:, 1:2]) * (1.0 / D) + half * half
    out[...] = ((resid[...] - mean) * lax.rsqrt(var + EPS_NORM) * gain[...] + bias[...]).astype(BF16)


def last_norm_body(resid, own, other, gain, bias, before, out):
    norm_body(resid, own, other, gain, bias, out)


def shape(rows, cols, dtype):
    return jax.ShapeDtypeStruct((rows, cols), dtype)


def layer(
    stream,
    w_pool_in,
    w_query,
    w_forget,
    w_value,
    w_outgate,
    pool_mix,
    pool_scale,
    lower_bound,
    extra_decay,
    rec_gain,
    w_out_pool,
    w_out_rec,
    norm_gain,
    norm_bias,
):
    xo = stream[0]
    length, half = xo.shape
    width = lower_bound.shape[0]
    heads = width // DK
    blocks = length // BLOCK
    pool_width = w_pool_in.shape[1]
    tile_gates, tile_pool, tile_query, tile_gate, tile_base = 1024, 1024, 1024, 1024, 1024
    sp_n = lax.axis_size(SP)
    tail = call(
        tail_body,
        (pltpu.with_memory_space_constraint(xo, pltpu.HBM),),
        [rows_spec(HALO, half, length // HALO - 1)],
        whole((HALO, half)),
        shape(HALO, half, BF16),
        (1,),
        vmem=4,
        flops=2 * length * D * width,
    )
    swap = [(0, 1), (1, 0)]
    pairs = [(0, 1), (1, 0), (2, 3), (3, 2)]
    mirror = [(0, 3), (3, 0), (1, 2), (2, 1)]

    xp = lax.ppermute(xo, "tp", swap)
    tail_o = lax.ppermute(tail, SP, [(i, i + 1) for i in range(sp_n - 1)])
    tail_p = lax.ppermute(tail_o, "tp", swap)

    full_flops = 2 * length * D * width
    halves = lambda rows: [rows_spec(rows, half), rows_spec(rows, half)]
    full_w = lambda cols: [whole((D, cols))]
    state_rows = blocks * width
    f_part = call(
        part_body,
        (xo, w_forget),
        [whole((length, half)), whole((D, width))],
        whole((length, width)),
        shape(length, width, F32),
        (1,),
        flops=full_flops // 2,
    )
    v = call(
        value_body,
        (xo, xp, w_value),
        halves(length) + full_w(width),
        whole((length, width)),
        shape(length, width, BF16),
        (1,),
        flops=full_flops,
    )
    down, rel, st, cfac, pay, own = call(
        functools.partial(gates_body, heads),
        (f_part, xp, w_forget, v, lower_bound.reshape(1, width), extra_decay.T),
        [rows_spec(tile_gates, width), rows_spec(tile_gates, half)]
        + full_w(width)
        + [
            rows_spec(tile_gates, width),
            whole((1, width)),
            pl.BlockSpec((heads, tile_gates), lambda i: (0, i)),
        ],
        [
            rows_spec(tile_gates, width),
            rows_spec(tile_gates, width),
            rows_spec(tile_gates // BLOCK * width, DK),
            whole((blocks, width)),
            whole((width + 16, DK)),
            whole((width + 8, DK)),
        ],
        [
            shape(length, width, BF16),
            shape(length, width, F32),
            shape(state_rows, DK, BF16),
            shape(blocks, width, F32),
            shape(width + 16, DK, BF16),
            shape(width + 8, DK, F32),
        ],
        (length // tile_gates,),
        scratch=[pltpu.VMEM((width, DK), F32), pltpu.VMEM((1, width), F32)],
        flops=full_flops,
    )

    def combine(which, *args):
        return call(
            functools.partial(combine_body, heads, which),
            args,
            [whole((width + 8, DK))] * (len(args) - 1) + [whole((width + 16, DK))],
            [whole((width + 16, DK))] + [whole((width + 8, DK))] * (2 - which // 2),
            [shape(width + 16, DK, BF16)] + [shape(width + 8, DK, F32)] * (2 - which // 2),
            (1,),
            vmem=4,
            flops=width * DK * 8,
        )

    got1 = lax.ppermute(pay, "sp_1", pairs)
    xo1, _ = lax.optimization_barrier((xo, pay))
    pool_o = call(
        functools.partial(pool_body, length),
        (xo1, xp, tail_o, tail_p, w_pool_in, pool_mix, pool_scale.reshape(1, pool_width)),
        halves(tile_pool)
        + [whole((HALO, half))] * 2
        + full_w(pool_width)
        + [whole(pool_mix.shape), whole((1, pool_width))],
        rows_spec(tile_pool, pool_width),
        shape(length, pool_width, BF16),
        (length // tile_pool,),
        scratch=[pltpu.VMEM((tile_pool + HALO, pool_width), BF16)],
        flops=full_flops,
    )
    pool_p = lax.ppermute(pool_o, "tp", swap)
    got1, pool_o1 = lax.optimization_barrier((got1, pool_o))
    pay2, pre2, own2 = combine(0, own, got1)

    got2 = lax.ppermute(pay2, "sp_1", mirror)
    rel1, _ = lax.optimization_barrier((rel, pay2))
    up, scores = call(
        functools.partial(query_body, heads),
        (xo, xp, w_query, rel1, down),
        halves(tile_query) + full_w(width) + [rows_spec(tile_query, width)] * 2,
        [rows_spec(tile_query, width)] * 2,
        [shape(length, width, BF16)] * 2,
        (length // tile_query,),
        flops=full_flops,
    )
    got2, up1 = lax.optimization_barrier((got2, up))
    pay3, pre3, own3 = combine(1, own2, pre2, got2)

    got3 = lax.ppermute(pay3, "sp_0", pairs)
    xo2, _ = lax.optimization_barrier((xo, pay3))
    gate = call(
        functools.partial(gate_body, heads),
        (xo2, xp, w_outgate, rec_gain.reshape(1, DK)),
        halves(tile_gate) + full_w(width) + [whole((1, DK))],
        rows_spec(tile_gate, width),
        shape(length, width, F32),
        (length // tile_gate,),
        flops=full_flops,
    )
    got3, gate1 = lax.optimization_barrier((got3, gate))
    pay4, pre4 = combine(2, own3, pre3, got3)

    got4 = lax.ppermute(pay4, "sp_0", mirror)
    wpool_p = lax.ppermute(w_out_pool, "tp", swap)
    wrec_p = lax.ppermute(w_out_rec, "tp", swap)
    pool_o2, _ = lax.optimization_barrier((pool_o1, pay4))
    base = call(
        pool_proj_body,
        (xo, pool_o2, pool_p, w_out_pool, wpool_p),
        [rows_spec(tile_base, half), rows_spec(tile_base, pool_width), rows_spec(tile_base, pool_width)]
        + [whole((pool_width, D))] * 2,
        rows_spec(tile_base, half),
        shape(length, half, F32),
        (length // tile_base,),
        flops=full_flops,
    )
    got4, base = lax.optimization_barrier((got4, base))

    parts = 2
    rows = length // parts
    tile = rows
    per_tile = tile // BLOCK
    per = rows // tile
    recs, others = [], []
    for part in range(parts):
        first = part * per
        rec = call(
            functools.partial(rec_body, heads, part * (blocks // parts)),
            (
                scores,
                up1,
                v,
                gate1,
                st,
                cfac,
                pre4,
                got4,
            ),
            [rows_spec(tile, width, first)] * 4
            + [
                rows_spec(per_tile * width, DK, first),
                whole((blocks, width)),
                whole((width + 8, DK)),
                whole((width + 16, DK)),
            ],
            rows_spec(tile, width),
            shape(rows, width, BF16),
            (per,),
            flops=full_flops // 4,
        )
        recs.append(rec)
        others.append(lax.ppermute(rec, "tp", swap))
    gain, bias = norm_gain.reshape(1, half), norm_bias.reshape(1, half)
    base_specs = lambda first: (
        [rows_spec(tile, half, first), rows_spec(tile, width), rows_spec(tile, width)]
        + [whole((width, D))] * 2
    )
    row_specs = [rows_spec(tile, half), rows_spec(tile, DK)]
    row_shapes = [shape(rows, half, F32), shape(rows, DK, F32)]
    resid0, stat0 = call(
        rec_proj_body,
        (base, recs[0], others[0], w_out_rec, wrec_p),
        base_specs(0),
        row_specs,
        row_shapes,
        (per,),
        flops=full_flops // 2,
    )
    stat0_p = lax.ppermute(stat0, "tp", swap)
    resid1, stat1 = call(
        rec_proj_body,
        (base, recs[1], others[1], w_out_rec, wrec_p),
        base_specs(per),
        row_specs,
        row_shapes,
        (per,),
        flops=full_flops // 2,
    )
    stat1_p = lax.ppermute(stat1, "tp", swap)
    resid0, _ = lax.optimization_barrier((resid0, stat1))
    fine = rows // 2
    norm_specs = [rows_spec(fine, half), rows_spec(fine, DK), rows_spec(fine, DK)] + [whole((1, half))] * 2
    out = call(
        norm_body,
        (resid0, stat0, stat0_p, gain, bias),
        norm_specs,
        rows_spec(fine, half),
        shape(length, half, BF16),
        (rows // fine,),
        flops=full_flops // 4,
    )
    out = call(
        last_norm_body,
        (resid1, stat1, stat1_p, gain, bias, out),
        norm_specs + [pl.BlockSpec(memory_space=pl.ANY)],
        rows_spec(fine, half, rows // fine),
        shape(length, half, BF16),
        (rows // fine,),
        flops=full_flops // 4,
        aliases={5: 0},
    )
    return out[None]


def solution(mesh):
    torus = Mesh(
        mesh.devices.reshape(4, 4, mesh.shape["fs"], mesh.shape["tp"]), ("sp_0", "sp_1", "fs", "tp")
    )
    return jax.shard_map(
        layer,
        mesh=torus,
        in_specs=(
            P("fs", SP, "tp"),
            P(None, "tp"),
            P(None, "tp"),
            P(None, "tp"),
            P(None, "tp"),
            P(None, "tp"),
            P("tp", None, None),
            P("tp"),
            P("tp"),
            P(SP, "tp"),
            P(),
            P("tp", None),
            P("tp", None),
            P("tp"),
            P("tp"),
        ),
        out_specs=P("fs", SP, "tp"),
        check_vma=False,
    )
```

```python
import functools

import jax
import jax.numpy as jnp
from jax import lax
from jax.experimental import pallas as pl
from jax.experimental.pallas import tpu as pltpu
from jax.sharding import Mesh
from jax.sharding import PartitionSpec as P

D = 2048
DK = 128
BLOCK = 128
MID = 63
VALUE_ROWS = 1024
HALO = 16
GROUP_CH = 256
SP = ("sp_0", "sp_1")
ALPHA = 2.0**0.25
EPS_RMS = 1e-06
EPS_NORM = 1e-05
F32 = jnp.float32
BF16 = jnp.bfloat16
MIB = 1 << 20


def mm(a, b):
    return jnp.dot(a, b, preferred_element_type=F32)


def mm_t(a, b, ca, cb):
    return lax.dot_general(a, b, (((ca,), (cb,)), ((), ())), preferred_element_type=F32)


def call(body, args, in_specs, out_specs, out_shape, grid, scratch=(), vmem=20, flops=0, aliases=None):
    nbytes = sum(a.size * a.dtype.itemsize for a in args)
    return pl.pallas_call(
        body,
        grid=grid,
        in_specs=in_specs,
        out_specs=out_specs,
        scratch_shapes=list(scratch),
        out_shape=out_shape,
        input_output_aliases=aliases or {},
        compiler_params=pltpu.CompilerParams(
            dimension_semantics=("arbitrary",) * len(grid), vmem_limit_bytes=vmem * MIB
        ),
        cost_estimate=pl.CostEstimate(flops=flops, bytes_accessed=nbytes, transcendentals=0),
    )(*args)


def rows_spec(rows, cols, first=0):
    return pl.BlockSpec((rows, cols), lambda i: (i + first, 0))


def whole(shape):
    return pl.BlockSpec(shape, lambda i: (0,) * len(shape))


def side(a, b):
    return jnp.concatenate([a, b], axis=1)


def stack(a, b):
    return jnp.concatenate([a, b], axis=0)


def own_cols(ref, cols):
    return ref[:, pl.ds(pl.multiple_of(lax.axis_index("tp") * cols, cols), cols)]


def own_then_other(ref):
    half = ref.shape[0] // 2
    k = lax.axis_index("tp")
    return stack(
        ref[pl.ds(pl.multiple_of(k * half, half), half), :],
        ref[pl.ds(pl.multiple_of((1 - k) * half, half), half), :],
    )


def later(which):
    place = lax.axis_index("sp_1" if which < 2 else "sp_0")
    return (place % 2 if which % 2 == 0 else place // 2) == 1


def tail_body(x, out):
    out[...] = x[...]


def half_rows(ref, which):
    half = ref.shape[0] // 2
    return ref[pl.ds(pl.multiple_of(which * half, half), half), :]


def part_body(xo, wf, out):
    out[...] = mm(xo[...], half_rows(wf, lax.axis_index("tp")))


def gates_body(heads, part, xo, xp, wf, wv, lb, ed, v, down_out, rel_out, st_out, c_out, pay_out, own_out, state, off):
    i = pl.program_id(0)
    rows = xp.shape[0]
    width = heads * DK

    @pl.when(i == 0)
    def _():
        state[...] = jnp.zeros_like(state)
        off[...] = jnp.zeros_like(off)

    f = (part[...] + mm(xp[...], half_rows(wf, 1 - lax.axis_index("tp")))).astype(BF16).astype(F32)
    low = lb[...]
    gap = 1.0 - low
    sig = jax.nn.sigmoid(f)
    weight = gap * (1.0 - sig)
    extra = ed[...]
    extra_hi = extra.astype(BF16).astype(F32)
    extra_rows = jnp.concatenate(
        [extra_hi, extra - extra_hi, jnp.zeros_like(extra), jnp.zeros_like(extra)], axis=0
    ).astype(BF16)
    row = lax.broadcasted_iota(jnp.int32, (4 * heads, width), 0)
    head = lax.broadcasted_iota(jnp.int32, (4 * heads, width), 1) // DK
    spread = ((row == head) | (row == head + heads)).astype(F32).astype(BF16)
    log_keep = jnp.log(low + gap * sig) + mm_t(extra_rows, spread, 0, 0)
    hi = log_keep.astype(BF16)
    lo = (log_keep - hi.astype(F32)).astype(BF16)
    t_id = lax.broadcasted_iota(jnp.int32, (BLOCK, 2 * BLOCK), 0)
    s_id = lax.broadcasted_iota(jnp.int32, (BLOCK, 2 * BLOCK), 1)
    mask = (t_id >= jnp.where(s_id >= BLOCK, s_id - BLOCK, s_id)).astype(F32).astype(BF16)
    per = VALUE_ROWS // BLOCK
    weights = []
    for b in range(rows // BLOCK):
        r = slice(b * BLOCK, (b + 1) * BLOCK)
        total = mm(mask, jnp.concatenate([hi[r], lo[r]], axis=0))
        middle = total[MID : MID + 1]
        end = total[BLOCK - 1 : BLOCK]
        rel = total - middle
        rel_out[r, :] = rel
        down = weight[r] * jnp.exp(-rel)
        down_out[r, :] = down.astype(BF16)
        before = off[...]
        c_out[pl.ds(i * (rows // BLOCK) + b, 1), :] = jnp.exp(middle + before)
        off[...] = before + end
        weights.append((b, (down * jnp.exp(end - middle)).astype(BF16), jnp.exp(middle), jnp.exp(end)))
        if len(weights) < per:
            continue
        some = slice((b + 1 - per) * BLOCK, (b + 1) * BLOCK)
        v[some, :] = mm(side(xo[some, :], xp[some, :]), own_then_other(wv)).astype(BF16)
        for at, in_weight, e_mid, e_end in weights:
            r = slice(at * BLOCK, (at + 1) * BLOCK)
            for h in range(heads):
                c = slice(h * DK, (h + 1) * DK)
                old = state[c, :]
                st_out[at * width + h * DK : at * width + (h + 1) * DK, :] = (old * e_mid[:, c]).astype(BF16)
                state[c, :] = old * e_end[:, c] + mm_t(v[r, c], in_weight[:, c], 0, 0)
        weights = []

    @pl.when(i == pl.num_programs(0) - 1)
    def _():
        write_payload(heads, state[...], jnp.exp(off[...]), pay_out, own_out)


def write_payload(heads, state, decay_row, pay_out, own_out):
    width = heads * DK
    decay = jnp.concatenate(
        [decay_row[:, h * DK : (h + 1) * DK] for h in range(heads)], axis=0
    )
    pack_payload(width, state, decay, pay_out)
    own_out[:width, :] = state
    own_out[width:, :] = jnp.concatenate([decay, jnp.zeros_like(decay)], axis=0)


def pack_payload(width, state, decay, pay_out):
    hi = decay.astype(BF16).astype(F32)
    pay_out[:width, :] = state.astype(BF16)
    pay_out[width:, :] = jnp.concatenate(
        [hi, decay - hi, jnp.zeros_like(hi), jnp.zeros_like(hi)], axis=0
    ).astype(BF16)


def unpack_decay(heads, width, ref):
    rows = ref[width:, :].astype(F32)
    return rows[:heads] + rows[heads : 2 * heads]


def combine_body(heads, which, own, *refs):
    width = heads * DK
    if which:
        pre, recv, pay_out, pre_out = refs[:4]
        own_out = refs[4] if len(refs) > 4 else None
    else:
        recv, pay_out, pre_out, own_out = refs
    early = later(which)
    d_own = own[width : width + heads, :]
    d_pre = pre[width : width + heads, :] if which else jnp.ones((heads, DK), F32)
    d_recv = unpack_decay(heads, width, recv)
    d_all = d_own * d_recv
    new_d_pre = jnp.where(early, d_recv * d_pre, d_pre)
    pre_out[width:, :] = jnp.concatenate([new_d_pre, jnp.zeros_like(d_pre)], axis=0)
    if own_out is not None:
        own_out[width:, :] = jnp.concatenate([d_all, jnp.zeros_like(d_all)], axis=0)
    states = []
    for h in range(heads):
        c = slice(h * DK, (h + 1) * DK)
        got = recv[c, :].astype(F32)
        mine = own[c, :]
        p = pre[c, :] if which else jnp.zeros((DK, DK), F32)
        pre_out[c, :] = jnp.where(early, p + d_pre[h : h + 1] * got, p)
        new = jnp.where(early, d_own[h : h + 1] * got + mine, d_recv[h : h + 1] * mine + got)
        if own_out is not None:
            own_out[c, :] = new
        states.append(new)
    pack_payload(width, jnp.concatenate(states, axis=0), d_all, pay_out)


def pool_body(length, xo, xp, to, tp, w, mix, scale, out, ext):
    i = pl.program_id(0)
    rows = xo.shape[0]

    @pl.when(i == 0)
    def _():
        ext[:HALO, :] = mm(side(to[...], tp[...]), own_then_other(w)).astype(BF16)

    @pl.when(i > 0)
    def _():
        ext[:HALO, :] = ext[rows : rows + HALO, :]

    ext[HALO:, :] = mm(side(xo[...], xp[...]), own_then_other(w)).astype(BF16)
    t_id = lax.broadcasted_iota(jnp.int32, (BLOCK, BLOCK + HALO), 0)
    s_id = lax.broadcasted_iota(jnp.int32, (BLOCK, BLOCK + HALO), 1)
    lag = t_id + HALO - s_id
    row_id = lax.broadcasted_iota(jnp.int32, (BLOCK, 1), 0)
    groups = mix.shape[0]
    for j in range(groups):
        window = jnp.left_shift(1, lax.axis_index("tp") * groups + j + 1)
        band = ((lag >= 0) & (lag < window)).astype(F32).astype(BF16)
        c = slice(j * GROUP_CH, (j + 1) * GROUP_CH)
        for b in range(rows // BLOCK):
            position = lax.axis_index(SP) * length + i * rows + b * BLOCK + row_id
            share = 1.0 / jnp.minimum(position + 1, window).astype(F32)
            sums = mm(band, ext[b * BLOCK : b * BLOCK + BLOCK + HALO, c])
            here = ext[b * BLOCK + HALO : b * BLOCK + BLOCK + HALO, c].astype(F32)
            diff = (sums * share - here).astype(BF16)
            out[b * BLOCK : (b + 1) * BLOCK, c] = (mm(diff, mix[j]) * scale[:, c]).astype(BF16)


def query_body(heads, xo, xp, w, rel, down, q_out, s_out):
    q = mm(side(xo[...], xp[...]), own_then_other(w)).astype(BF16).astype(F32)
    up = (jax.nn.silu(q) * jnp.exp(rel[...])).astype(BF16)
    q_out[...] = up
    t_id = lax.broadcasted_iota(jnp.int32, (BLOCK, BLOCK), 0)
    s_id = lax.broadcasted_iota(jnp.int32, (BLOCK, BLOCK), 1)
    keep = t_id >= s_id
    for b in range(up.shape[0] // BLOCK):
        r = slice(b * BLOCK, (b + 1) * BLOCK)
        for h in range(heads):
            c = slice(h * DK, (h + 1) * DK)
            score = mm_t(up[r, c], down[r, c], 1, 1)
            s_out[r, c] = jnp.where(keep, score, 0.0).astype(BF16)


def gate_body(heads, xo, xp, w, gain, out):
    g = mm(side(xo[...], xp[...]), own_then_other(w)).astype(BF16).astype(F32)
    out[...] = jax.nn.silu(g) * jnp.concatenate([gain[...]] * heads, axis=1)


def rec_body(heads, start, scores, up, v, gate, st, cfac, pre, recv, out):
    width = heads * DK
    early = later(3)
    factor = jnp.where(early, 1.0, 0.0)
    rows = up.shape[0]
    first = start + pl.program_id(0) * (rows // BLOCK)
    for h in range(heads):
        c = slice(h * DK, (h + 1) * DK)
        coming = pre[c, :] + (pre[width + h : width + h + 1, :] * factor) * recv[c, :].astype(F32)
        for b in range(rows // BLOCK):
            r = slice(b * BLOCK, (b + 1) * BLOCK)
            base = b * width + h * DK
            scale = cfac[pl.ds(first + b, 1), :][:, c]
            full = (st[base : base + DK, :].astype(F32) + scale * coming).astype(BF16)
            raw = mm(scores[r, c], v[r, c]) + mm_t(up[r, c], full, 1, 1)
            mean = jnp.mean(raw * raw, axis=-1, keepdims=True)
            out[r, c] = (raw * lax.rsqrt(mean + EPS_RMS) * gate[r, c]).astype(BF16)


def pool_proj_body(x, po, pp, wo, wp, out):
    cols = out.shape[1]
    out[...] = ALPHA * x[...].astype(F32) + mm(
        side(po[...], pp[...]), stack(own_cols(wo, cols), own_cols(wp, cols))
    )


def rec_proj_body(base, ro, rp, wo, wp, out, stats):
    cols = out.shape[1]
    resid = base[...] + mm(side(ro[...], rp[...]), stack(own_cols(wo, cols), own_cols(wp, cols)))
    out[...] = resid
    mean = jnp.mean(resid, axis=-1, keepdims=True)
    dev = resid - mean
    spread = jnp.sum(dev * dev, axis=-1, keepdims=True)
    lane = lax.broadcasted_iota(jnp.int32, (resid.shape[0], DK), 1)
    stats[...] = jnp.where(lane == 0, mean, spread)


def norm_body(resid, own, other, gain, bias, out):
    a, b = own[...], other[...]
    mean_a, mean_b = a[:, 0:1], b[:, 0:1]
    mean = 0.5 * (mean_a + mean_b)
    half = 0.5 * (mean_a - mean_b)
    var = (a[:, 1:2] + b[:, 1:2]) * (1.0 / D) + half * half
    out[...] = ((resid[...] - mean) * lax.rsqrt(var + EPS_NORM) * gain[...] + bias[...]).astype(BF16)


def last_norm_body(resid, own, other, gain, bias, before, out):
    norm_body(resid, own, other, gain, bias, out)


def shape(rows, cols, dtype):
    return jax.ShapeDtypeStruct((rows, cols), dtype)


def layer(
    stream,
    w_pool_in,
    w_query,
    w_forget,
    w_value,
    w_outgate,
    pool_mix,
    pool_scale,
    lower_bound,
    extra_decay,
    rec_gain,
    w_out_pool,
    w_out_rec,
    norm_gain,
    norm_bias,
):
    xo = stream[0]
    length, half = xo.shape
    width = lower_bound.shape[0]
    heads = width // DK
    blocks = length // BLOCK
    pool_width = w_pool_in.shape[1]
    tile_gates, tile_pool, tile_query, tile_gate, tile_base = 1024, 1024, 1024, 1024, 1024
    sp_n = lax.axis_size(SP)
    tail = call(
        tail_body,
        (pltpu.with_memory_space_constraint(xo, pltpu.HBM),),
        [rows_spec(HALO, half, length // HALO - 1)],
        whole((HALO, half)),
        shape(HALO, half, BF16),
        (1,),
        vmem=4,
        flops=2 * length * D * width,
    )
    swap = [(0, 1), (1, 0)]
    pairs = [(0, 1), (1, 0), (2, 3), (3, 2)]
    mirror = [(0, 3), (3, 0), (1, 2), (2, 1)]

    xp = lax.ppermute(xo, "tp", swap)
    tail_o = lax.ppermute(tail, SP, [(i, i + 1) for i in range(sp_n - 1)])
    tail_p = lax.ppermute(tail_o, "tp", swap)

    full_flops = 2 * length * D * width
    halves = lambda rows: [rows_spec(rows, half), rows_spec(rows, half)]
    full_w = lambda cols: [whole((D, cols))]
    state_rows = blocks * width
    f_part = call(
        part_body,
        (xo, w_forget),
        [whole((length, half)), whole((D, width))],
        whole((length, width)),
        shape(length, width, F32),
        (1,),
        flops=full_flops // 2,
    )
    v, down, rel, st, cfac, pay, own = call(
        functools.partial(gates_body, heads),
        (f_part, xo, xp, w_forget, w_value, lower_bound.reshape(1, width), extra_decay.T),
        [rows_spec(tile_gates, width)]
        + halves(tile_gates)
        + full_w(width) * 2
        + [
            whole((1, width)),
            pl.BlockSpec((heads, tile_gates), lambda i: (0, i)),
        ],
        [
            rows_spec(tile_gates, width),
            rows_spec(tile_gates, width),
            rows_spec(tile_gates, width),
            rows_spec(tile_gates // BLOCK * width, DK),
            whole((blocks, width)),
            whole((width + 16, DK)),
            whole((width + 8, DK)),
        ],
        [
            shape(length, width, BF16),
            shape(length, width, BF16),
            shape(length, width, F32),
            shape(state_rows, DK, BF16),
            shape(blocks, width, F32),
            shape(width + 16, DK, BF16),
            shape(width + 8, DK, F32),
        ],
        (length // tile_gates,),
        scratch=[pltpu.VMEM((width, DK), F32), pltpu.VMEM((1, width), F32)],
        flops=full_flops,
    )

    def combine(which, *args):
        return call(
            functools.partial(combine_body, heads, which),
            args,
            [whole((width + 8, DK))] * (len(args) - 1) + [whole((width + 16, DK))],
            [whole((width + 16, DK))] + [whole((width + 8, DK))] * (2 - which // 2),
            [shape(width + 16, DK, BF16)] + [shape(width + 8, DK, F32)] * (2 - which // 2),
            (1,),
            vmem=4,
            flops=width * DK * 8,
        )

    got1 = lax.ppermute(pay, "sp_1", pairs)
    xo1, _ = lax.optimization_barrier((xo, pay))
    pool_o = call(
        functools.partial(pool_body, length),
        (xo1, xp, tail_o, tail_p, w_pool_in, pool_mix, pool_scale.reshape(1, pool_width)),
        halves(tile_pool)
        + [whole((HALO, half))] * 2
        + full_w(pool_width)
        + [whole(pool_mix.shape), whole((1, pool_width))],
        rows_spec(tile_pool, pool_width),
        shape(length, pool_width, BF16),
        (length // tile_pool,),
        scratch=[pltpu.VMEM((tile_pool + HALO, pool_width), BF16)],
        flops=full_flops,
    )
    pool_p = lax.ppermute(pool_o, "tp", swap)
    got1, pool_o1 = lax.optimization_barrier((got1, pool_o))
    pay2, pre2, own2 = combine(0, own, got1)

    got2 = lax.ppermute(pay2, "sp_1", mirror)
    rel1, _ = lax.optimization_barrier((rel, pay2))
    up, scores = call(
        functools.partial(query_body, heads),
        (xo, xp, w_query, rel1, down),
        halves(tile_query) + full_w(width) + [rows_spec(tile_query, width)] * 2,
        [rows_spec(tile_query, width)] * 2,
        [shape(length, width, BF16)] * 2,
        (length // tile_query,),
        flops=full_flops,
    )
    got2, up1 = lax.optimization_barrier((got2, up))
    pay3, pre3, own3 = combine(1, own2, pre2, got2)

    got3 = lax.ppermute(pay3, "sp_0", pairs)
    xo2, _ = lax.optimization_barrier((xo, pay3))
    gate = call(
        functools.partial(gate_body, heads),
        (xo2, xp, w_outgate, rec_gain.reshape(1, DK)),
        halves(tile_gate) + full_w(width) + [whole((1, DK))],
        rows_spec(tile_gate, width),
        shape(length, width, F32),
        (length // tile_gate,),
        flops=full_flops,
    )
    got3, gate1 = lax.optimization_barrier((got3, gate))
    pay4, pre4 = combine(2, own3, pre3, got3)

    got4 = lax.ppermute(pay4, "sp_0", mirror)
    wpool_p = lax.ppermute(w_out_pool, "tp", swap)
    wrec_p = lax.ppermute(w_out_rec, "tp", swap)
    pool_o2, _ = lax.optimization_barrier((pool_o1, pay4))
    base = call(
        pool_proj_body,
        (xo, pool_o2, pool_p, w_out_pool, wpool_p),
        [rows_spec(tile_base, half), rows_spec(tile_base, pool_width), rows_spec(tile_base, pool_width)]
        + [whole((pool_width, D))] * 2,
        rows_spec(tile_base, half),
        shape(length, half, F32),
        (length // tile_base,),
        flops=full_flops,
    )
    got4, base = lax.optimization_barrier((got4, base))

    parts = 2
    rows = length // parts
    tile = rows
    per_tile = tile // BLOCK
    per = rows // tile
    recs, others = [], []
    for part in range(parts):
        first = part * per
        rec = call(
            functools.partial(rec_body, heads, part * (blocks // parts)),
            (
                scores,
                up1,
                v,
                gate1,
                st,
                cfac,
                pre4,
                got4,
            ),
            [rows_spec(tile, width, first)] * 4
            + [
                rows_spec(per_tile * width, DK, first),
                whole((blocks, width)),
                whole((width + 8, DK)),
                whole((width + 16, DK)),
            ],
            rows_spec(tile, width),
            shape(rows, width, BF16),
            (per,),
            flops=full_flops // 4,
        )
        recs.append(rec)
        others.append(lax.ppermute(rec, "tp", swap))
    gain, bias = norm_gain.reshape(1, half), norm_bias.reshape(1, half)
    base_specs = lambda first: (
        [rows_spec(tile, half, first), rows_spec(tile, width), rows_spec(tile, width)]
        + [whole((width, D))] * 2
    )
    row_specs = [rows_spec(tile, half), rows_spec(tile, DK)]
    row_shapes = [shape(rows, half, F32), shape(rows, DK, F32)]
    resid0, stat0 = call(
        rec_proj_body,
        (base, recs[0], others[0], w_out_rec, wrec_p),
        base_specs(0),
        row_specs,
        row_shapes,
        (per,),
        flops=full_flops // 2,
    )
    stat0_p = lax.ppermute(stat0, "tp", swap)
    resid1, stat1 = call(
        rec_proj_body,
        (base, recs[1], others[1], w_out_rec, wrec_p),
        base_specs(per),
        row_specs,
        row_shapes,
        (per,),
        flops=full_flops // 2,
    )
    stat1_p = lax.ppermute(stat1, "tp", swap)
    resid0, _ = lax.optimization_barrier((resid0, stat1))
    fine = rows // 2
    norm_specs = [rows_spec(fine, half), rows_spec(fine, DK), rows_spec(fine, DK)] + [whole((1, half))] * 2
    out = call(
        norm_body,
        (resid0, stat0, stat0_p, gain, bias),
        norm_specs,
        rows_spec(fine, half),
        shape(length, half, BF16),
        (rows // fine,),
        flops=full_flops // 4,
    )
    out = call(
        last_norm_body,
        (resid1, stat1, stat1_p, gain, bias, out),
        norm_specs + [pl.BlockSpec(memory_space=pl.ANY)],
        rows_spec(fine, half, rows // fine),
        shape(length, half, BF16),
        (rows // fine,),
        flops=full_flops // 4,
        aliases={5: 0},
    )
    return out[None]


def solution(mesh):
    torus = Mesh(
        mesh.devices.reshape(4, 4, mesh.shape["fs"], mesh.shape["tp"]), ("sp_0", "sp_1", "fs", "tp")
    )
    return jax.shard_map(
        layer,
        mesh=torus,
        in_specs=(
            P("fs", SP, "tp"),
            P(None, "tp"),
            P(None, "tp"),
            P(None, "tp"),
            P(None, "tp"),
            P(None, "tp"),
            P("tp", None, None),
            P("tp"),
            P("tp"),
            P(SP, "tp"),
            P(),
            P("tp", None),
            P("tp", None),
            P("tp"),
            P("tp"),
        ),
        out_specs=P("fs", SP, "tp"),
        check_vma=False,
    )
```
